256 devices in a mesh: sp: 32 (over z, x), tp: 8 (over y, core).
Axes of the slice: x: 4, y: 4, z: 8, core: 2. Of those that a mesh axis runs over, the one named last changes fastest.
Arguments:
- latents: bfloat16 [16384, 2048], P(('sp', 'tp')), may hold values from -6 to 6
- context: bfloat16 [512, 2048], P('sp'), may hold values from -6 to 6
- cond: float32 [2048], P('sp'), may hold values from -6 to 6
- ctx_cond: float32 [2048], P('sp'), may hold values from -6 to 6
- mod_weight: float32 [2048, 6144], P('sp', 'tp'), may hold values from -0.125 to 0.125
- query_weight: bfloat16 [2048, 2048], P(None, 'tp'), may hold values from -1 to 1, as said below
- key_matrix: bfloat16 [2048, 1024], P(None, 'tp'), may hold values from -1 to 1, as said below
- value_matrix: bfloat16 [2048, 1024], P(None, 'tp'), may hold values from -0.125 to 0.125
- out_weight: bfloat16 [2048, 2048], P('tp'), may hold values from -0.125 to 0.125
- query_gain: float32 [128], replicated, may hold values from 0.7 to 7
- key_gain: float32 [128], replicated, may hold values from 0.7 to 7
Outputs:
- updated: bfloat16 [16384, 2048], P(('sp', 'tp'))
The draws below stay inside these ranges and needn't reach their ends.
Inputs may be any that keep to these rules, and one draw needn't show every extreme that they name: `query_weight`: entries of order 2048 to the power -1/2. `key_matrix`: entries of order 2048 to the power -1/2.
All inputs are finite; a program needn't handle non-finite values.
Results may differ from the reference program's by a relative error of at most 0.0085.
The reference program's roundings to bfloat16 on the way count: a program that leaves them out, or rounds other values in their place, can miss the bound.
Values may be sent and summed in bfloat16 or wider, within the bound.
A program may use at most 128 MiB of HBM per device.

```python
import math
import jax
import jax.numpy as jnp
from jax import lax

MODEL_DIM = 2048
HEAD_SIZE = 128
QUERY_HEAD_COUNT = 16
KEY_VALUE_HEADS = 8
GRID_W = 64
CTX = 512
TOKENS = 16384


def paired_weights(key):
    query_base = jax.random.normal(jax.random.fold_in(key, 11), (MODEL_DIM, QUERY_HEAD_COUNT * HEAD_SIZE), jnp.float32) * MODEL_DIM ** (-0.5)
    key_start = jax.random.normal(jax.random.fold_in(key, 12), (MODEL_DIM, KEY_VALUE_HEADS * HEAD_SIZE), jnp.float32) * MODEL_DIM ** (-0.5)
    return (query_base, key_start)


def draw_query_weight(key, part):
    return paired_weights(key)[0].astype(jnp.bfloat16)


def draw_key_matrix(key, part):
    return paired_weights(key)[1].astype(jnp.bfloat16)


def draw_query_gain(key, part):
    return jax.random.uniform(jax.random.fold_in(key, 21), (HEAD_SIZE,), jnp.float32, 0.7, 1.3)


def draw_key_gain(key, part):
    return jax.random.uniform(jax.random.fold_in(key, 22), (HEAD_SIZE,), jnp.float32, 0.7, 1.3)


def shard_levels(rng, dims, shards, smallest, high):
    loudness, own = 1.0, jax.random.fold_in(rng, 6)
    for position, parts in shards:
        draws = jnp.exp(jax.random.uniform(jax.random.fold_in(own, position), (parts,), jnp.float32, smallest / len(shards), high / len(shards)))
        loudness = loudness * jnp.repeat(draws, dims[position] // parts).reshape([-1 if axis == position else 1 for axis in range(len(dims))])
    return loudness


def centred(stream_key, dims, width, most, pieces=(), kind=jnp.bfloat16):
    result = jax.random.normal(stream_key, dims, jnp.float32) * width
    if len(pieces) > 0:
        result = shard_levels(stream_key, dims, pieces, -0.22, 0.18) * result
    return jnp.clip(result, min=-most, max=most).astype(kind)


def setup_inputs(seed: int = 0) -> dict:
    key_of = jax.random.split(jax.random.key(seed), 12)
    latents = centred(key_of[0], (TOKENS, MODEL_DIM), 1.0, 6.0, ((0, 256),))
    context = centred(key_of[1], (CTX, MODEL_DIM), 1.0, 6.0, ((0, 32),))
    cond = centred(key_of[2], (MODEL_DIM,), 1.0, 6.0, ((0, 32),), jnp.float32)
    ctx_cond = centred(key_of[3], (MODEL_DIM,), 1.0, 6.0, ((0, 32),), jnp.float32)
    mod_weight = centred(key_of[4], (MODEL_DIM, 3 * MODEL_DIM), MODEL_DIM ** -0.5, 0.125, ((0, 32), (1, 8)), jnp.float32)
    query_weight = draw_query_weight(jax.random.fold_in(key_of[11], 71), 0)
    key_matrix = draw_key_matrix(jax.random.fold_in(key_of[11], 71), 0)
    value_matrix = centred(key_of[7], (MODEL_DIM, KEY_VALUE_HEADS * HEAD_SIZE), MODEL_DIM ** -0.5, 0.125, ((1, 8),))
    out_weight = centred(key_of[8], (QUERY_HEAD_COUNT * HEAD_SIZE, MODEL_DIM), (QUERY_HEAD_COUNT * HEAD_SIZE) ** -0.5, 0.125, ((0, 8),))
    query_gain = draw_query_gain(jax.random.fold_in(key_of[11], 71), 0)
    key_gain = draw_key_gain(jax.random.fold_in(key_of[11], 71), 0)
    return {"latents": latents, "context": context, "cond": cond, "ctx_cond": ctx_cond, "mod_weight": mod_weight, "query_weight": query_weight, "key_matrix": key_matrix, "value_matrix": value_matrix, "out_weight": out_weight, "query_gain": query_gain, "key_gain": key_gain}


NORM_EPS = 1e-06
ROPE_BASE = 10000.0

def normalize(latent_value_rows):
    return latent_value_rows * lax.rsqrt(lax.optimization_barrier(jnp.mean(latent_value_rows * latent_value_rows, axis=-1, keepdims=True)) + NORM_EPS)

def rotate(latent_value_rows, positions):
    quarter = latent_value_rows.shape[-1] // 2
    inv_freq = ROPE_BASE ** (-jnp.arange(quarter, dtype=jnp.float32) / quarter)
    angles = positions.astype(jnp.float32)[:, None] * inv_freq[None, :]
    cos_table = jnp.cos(angles)[:, None, :]
    sin_table = jnp.sin(angles)[:, None, :]
    first, second = (latent_value_rows[..., :quarter], latent_value_rows[..., quarter:])
    return jnp.concatenate([first * cos_table - second * sin_table, second * cos_table + first * sin_table], axis=-1)

def axial(latent_value_rows, positions):
    half_dim = latent_value_rows.shape[-1] // 2
    return jnp.concatenate([rotate(latent_value_rows[..., :half_dim], positions // GRID_W), rotate(latent_value_rows[..., half_dim:], positions % GRID_W)], axis=-1)

def modulate(latent_value_rows, mod_row):
    model_width = latent_value_rows.shape[-1]
    shift_vec = mod_row[:model_width]
    scale_vec = mod_row[model_width:2 * model_width]
    return (normalize(latent_value_rows.astype(jnp.float32)) * (1.0 + scale_vec) + shift_vec).astype(jnp.bfloat16)

def reference(latents, context, cond, ctx_cond, mod_weight, query_weight, key_matrix, value_matrix, out_weight, query_gain, key_gain):
    model_width = latents.shape[1]
    latent_count = latents.shape[0]
    prefix_count = context.shape[0]
    modulation = jnp.dot(jax.nn.silu(jnp.stack([cond, ctx_cond])), mod_weight, precision=lax.Precision.HIGHEST)
    gate_vec = modulation[0, 2 * model_width:]
    normalised_rows = modulate(latents, modulation[0])
    prefix_normalised = modulate(context, modulation[1])
    positions = jnp.arange(latent_count, dtype=jnp.int32)
    query_rows = jnp.dot(normalised_rows, query_weight, preferred_element_type=jnp.float32).reshape(latent_count, QUERY_HEAD_COUNT, HEAD_SIZE)
    query_rows = axial(normalize(query_rows) * query_gain, positions).astype(jnp.bfloat16)
    latent_key_rows = jnp.dot(normalised_rows, key_matrix, preferred_element_type=jnp.float32).reshape(latent_count, KEY_VALUE_HEADS, HEAD_SIZE)
    latent_key_rows = axial(normalize(latent_key_rows) * key_gain, positions).astype(jnp.bfloat16)
    latent_value_rows = jnp.dot(normalised_rows, value_matrix, preferred_element_type=jnp.float32).reshape(latent_count, KEY_VALUE_HEADS, HEAD_SIZE).astype(jnp.bfloat16)
    prefix_keys = jnp.dot(prefix_normalised, key_matrix, preferred_element_type=jnp.float32).reshape(prefix_count, KEY_VALUE_HEADS, HEAD_SIZE)
    prefix_keys = (normalize(prefix_keys) * key_gain).astype(jnp.bfloat16)
    prefix_values = jnp.dot(prefix_normalised, value_matrix, preferred_element_type=jnp.float32).reshape(prefix_count, KEY_VALUE_HEADS, HEAD_SIZE).astype(jnp.bfloat16)
    keys_all = jnp.concatenate([prefix_keys, latent_key_rows], axis=0).astype(jnp.float32)
    values_all = jnp.concatenate([prefix_values, latent_value_rows], axis=0).astype(jnp.float32)
    lift = math.log(latent_count / (2.0 * prefix_count))
    lift_row = jnp.concatenate([jnp.full((prefix_count,), lift, jnp.float32), jnp.zeros((latent_count,), jnp.float32)])
    group_size = QUERY_HEAD_COUNT // KEY_VALUE_HEADS
    rows_per_block = math.gcd(latent_count, 256)
    token_blocks = query_rows.reshape(latent_count // rows_per_block, rows_per_block, KEY_VALUE_HEADS, group_size, HEAD_SIZE)
    inv_root = HEAD_SIZE ** (-0.5)

    def one_block(block):
        scores = jnp.einsum('qhgd,khd->hgqk', block.astype(jnp.float32), keys_all) * inv_root + lift_row
        top_row = lax.optimization_barrier(jnp.max(scores, axis=-1, keepdims=True))
        weights = jnp.exp(scores - top_row)
        total = lax.optimization_barrier(jnp.sum(weights, axis=-1))
        probs = lax.optimization_barrier(weights.astype(jnp.bfloat16)).astype(jnp.float32)
        summed = jnp.einsum('hgqk,khd->qhgd', probs, values_all)
        return (summed / jnp.transpose(total, (2, 0, 1))[..., None]).astype(jnp.bfloat16)
    attended = lax.map(one_block, token_blocks).reshape(latent_count, QUERY_HEAD_COUNT * HEAD_SIZE)
    mixed = jnp.dot(attended, out_weight, preferred_element_type=jnp.float32)
    return (latents.astype(jnp.float32) + gate_vec * normalize(mixed)).astype(jnp.bfloat16)
```

```python
import functools
import math

import jax
import jax.numpy as jnp
import numpy as np
from jax import lax
from jax.experimental import pallas as pl
from jax.experimental.pallas import tpu as pltpu
from jax.sharding import Mesh
from jax.sharding import PartitionSpec as P

MESH_ID = pl.DeviceIdType.MESH
GRID_W = 64
NORM_EPS = 1e-06
ROPE_BASE = 10000.0
NZ, NX, NY, NC = 8, 4, 4, 2
NTP = NY * NC
BF16, F32 = jnp.bfloat16, jnp.float32
VMEM_SPEC = pl.BlockSpec(memory_space=pltpu.VMEM)


def remote(src, dst, send_sem, recv_sem, **to):
    return pltpu.make_async_remote_copy(
        src_ref=src,
        dst_ref=dst,
        send_sem=send_sem,
        recv_sem=recv_sem,
        device_id=to,
        device_id_type=MESH_ID,
    )


def greet(peers):
    barrier = pltpu.get_barrier_semaphore()
    for peer in peers:
        pl.semaphore_signal(barrier, inc=1, device_id=peer, device_id_type=MESH_ID)
    pl.semaphore_wait(barrier, len(peers))


def tp_peers(y, c):
    peers = [{"c": 1 - c}]
    for dy in range(1, NY):
        for dc in range(NC):
            peers.append({"y": lax.rem(y + dy, NY), "c": lax.rem(c + dc, NC)})
    return peers


def tp_index(peer, y, c):
    return peer.get("y", y) * NC + peer["c"]


def diagonal(n):
    return lax.broadcasted_iota(jnp.int32, (n, n), 0) == lax.broadcasted_iota(jnp.int32, (n, n), 1)


def gather_kernel(
    lat, cond, ctx_cond, mod_weight, rows, mod, part, px, pt, zbuf, xbuf, tbuf, rs, rr, zs, zr, xs, xr, ts, tr
):
    z, x, y, c = (lax.axis_index(a) for a in ("z", "x", "y", "c"))
    me = y * NC + c
    yp, ym = lax.rem(y + 1, NY), lax.rem(y + NY - 1, NY)
    n = lat.shape[0]
    half = n // 2
    z_to = [{"z": lax.rem(z + d, NZ)} for d in range(1, NZ)]
    x_to = [{"x": lax.rem(x + d, NX)} for d in range(1, NX)]
    t_to = tp_peers(y, c)
    greet(z_to + x_to + t_to)

    up = remote(lat, rows.at[me], rs.at[0], rr.at[0], y=yp)
    down = remote(lat, rows.at[me], rs.at[1], rr.at[1], y=ym)
    over = remote(lat, rows.at[me], rs.at[2], rr.at[2], c=1 - c)
    up.start()
    down.start()
    over.start()

    eye = diagonal(cond.shape[1])
    for r, ref in enumerate((cond, ctx_cond)):
        v = ref[...]
        v = v * jax.nn.sigmoid(v)
        column = jnp.sum(jnp.where(eye, jnp.broadcast_to(v, eye.shape), 0.0), axis=1, keepdims=True)
        part[r : r + 1, :] = jnp.sum(column * mod_weight[...], axis=0, keepdims=True)
    z_out = [remote(part, zbuf.at[z], zs.at[i], zr.at[i], **to) for i, to in enumerate(z_to)]
    for cp in z_out:
        cp.start()
    zbuf[z] = part[...]
    rows[me] = lat[...]
    for cp in z_out:
        cp.wait_recv()
    px[...] = sum((zbuf[i] for i in range(1, NZ)), zbuf[0])
    x_out = [remote(px, xbuf.at[x], xs.at[i], xr.at[i], **to) for i, to in enumerate(x_to)]
    for cp in x_out:
        cp.start()
    xbuf[x] = px[...]

    up.wait_recv()
    down.wait_recv()
    low, high = ym * NC + c, yp * NC + c
    far = lax.rem(y + 2, NY) * NC + c
    up2 = remote(rows.at[low, 0:half], rows.at[low, 0:half], rs.at[3], rr.at[3], y=yp)
    down2 = remote(rows.at[high, half:n], rows.at[high, half:n], rs.at[4], rr.at[4], y=ym)
    up2.start()
    down2.start()
    over1 = remote(rows.at[low], rows.at[low], rs.at[5], rr.at[5], c=1 - c)
    over2 = remote(rows.at[high], rows.at[high], rs.at[6], rr.at[6], c=1 - c)
    over1.start()
    over2.start()

    for cp in x_out:
        cp.wait_recv()
    pt[...] = sum((xbuf[i] for i in range(1, NX)), xbuf[0])
    t_out = [remote(pt, tbuf.at[me], ts.at[i], tr.at[i], **to) for i, to in enumerate(t_to)]
    for cp in t_out:
        cp.start()
    tbuf[me] = pt[...]

    up2.wait_recv()
    down2.wait_recv()
    over3 = remote(rows.at[far], rows.at[far], rs.at[7], rr.at[7], c=1 - c)
    over3.start()
    for cp in t_out:
        cp.wait_recv()
    w = part.shape[1]
    for i in range(NTP):
        mod[:, i * w : (i + 1) * w] = tbuf[i]
    for cp in (over, over1, over2, over3):
        cp.wait_recv()
    for cp in [up, down, over, up2, down2, over1, over2, over3] + z_out + x_out + t_out:
        cp.wait_send()


def gather_stage(latents, cond, ctx_cond, mod_weight):
    n, d = latents.shape
    cols = mod_weight.shape[1]
    dma = pltpu.SemaphoreType.DMA
    return pl.pallas_call(
        gather_kernel,
        name="gather_stage",
        out_shape=(
            jax.ShapeDtypeStruct((NTP, n, d), BF16),
            jax.ShapeDtypeStruct((2, NTP * cols), F32),
        ),
        in_specs=[VMEM_SPEC] * 4,
        out_specs=(VMEM_SPEC, VMEM_SPEC),
        scratch_shapes=[
            pltpu.VMEM((2, cols), F32),
            pltpu.VMEM((2, cols), F32),
            pltpu.VMEM((2, cols), F32),
            pltpu.VMEM((NZ, 2, cols), F32),
            pltpu.VMEM((NX, 2, cols), F32),
            pltpu.VMEM((NTP, 2, cols), F32),
            dma((8,)),
            dma((8,)),
            dma((NZ - 1,)),
            dma((NZ - 1,)),
            dma((NX - 1,)),
            dma((NX - 1,)),
            dma((NTP - 1,)),
            dma((NTP - 1,)),
        ],
        compiler_params=pltpu.CompilerParams(collective_id=0, has_side_effects=True),
    )(latents, cond[None, :], ctx_cond[None, :], mod_weight)


def rope_tables(row_tokens, freqs):
    c = freqs // 4
    inv = (ROPE_BASE ** (-np.arange(c, dtype=np.float32) / np.float32(c))).astype(np.float32)

    def table(count, lanes_from):
        angles = np.arange(count, dtype=np.float32)[:, None] * inv[None, :]
        cos, sin = np.cos(angles), np.sin(angles)
        out_c = np.zeros((count, freqs), np.float32)
        out_s = np.zeros((count, freqs), np.float32)
        out_c[:, lanes_from : lanes_from + 2 * c] = np.concatenate([cos, cos], 1)
        out_s[:, lanes_from : lanes_from + 2 * c] = np.concatenate([-sin, sin], 1)
        return out_c, out_s

    return table(row_tokens, 0) + table(GRID_W, freqs // 2)


def rms(v):
    return v * lax.rsqrt(jnp.mean(v * v, axis=-1, keepdims=True) + NORM_EPS)


def project_kernel(rows, ctx, mod, wq, wk, wv, qg, kg, row_c, row_s, col_c, col_s, q_out, kv_out):
    step = pl.program_id(0)
    d = wq.shape[0]
    hd = wk.shape[1]
    count = rows.shape[0] * rows.shape[1]
    n_ctx = ctx.shape[0]
    sp = lax.axis_index("z") * NX + lax.axis_index("x")
    groups = count // GRID_W

    def modulated(v, r):
        v = rms(v.astype(F32))
        return (v * (1.0 + mod[r : r + 1, d : 2 * d]) + mod[r : r + 1, 0:d]).astype(BF16)

    steps = pl.num_programs(0)
    first = (sp * steps + step) * groups
    cos = jnp.concatenate([row_c[pl.ds(first + g, 1), :] + col_c[...] for g in range(groups)], axis=0)
    sin = jnp.concatenate([row_s[pl.ds(first + g, 1), :] + col_s[...] for g in range(groups)], axis=0)
    lane = lax.broadcasted_iota(jnp.int32, (count, hd), 1)
    early = lax.rem(lane, hd // 2) < hd // 4

    def turned(v):
        other = jnp.where(early, pltpu.roll(v, hd - hd // 4, 1), pltpu.roll(v, hd // 4, 1))
        return v * cos + other * sin

    a = modulated(rows[...].reshape(count, d), 0)
    q = jnp.dot(a, wq[...], preferred_element_type=F32)
    k = jnp.dot(a, wk[...], preferred_element_type=F32)
    v = jnp.dot(a, wv[...], preferred_element_type=F32)
    at = pl.multiple_of(step * count, count)
    for h in range(q_out.shape[0]):
        q_out[h, pl.ds(at, count), :] = turned(rms(q[:, h * hd : (h + 1) * hd]) * qg[...]).astype(BF16)
    kv_out[pl.ds(at, count), 0:hd] = turned(rms(k) * kg[...]).astype(BF16)
    kv_out[pl.ds(at, count), hd : 2 * hd] = v.astype(BF16)

    @pl.when(step == 0)
    def _():
        b = modulated(ctx[...], 1)
        kc = jnp.dot(b, wk[...], preferred_element_type=F32)
        vc = jnp.dot(b, wv[...], preferred_element_type=F32)
        end = kv_out.shape[0]
        kv_out[end - n_ctx : end, 0:hd] = (rms(kc) * kg[...]).astype(BF16)
        kv_out[end - n_ctx : end, hd : 2 * hd] = vc.astype(BF16)


def project_stage(rows, ctx, mod, wq, wk, wv, qg, kg):
    ntp, n, d = rows.shape
    hd = qg.shape[0]
    heads = wq.shape[1] // hd
    total = ntp * n
    steps = 2
    tables = rope_tables(NZ * NX * total // GRID_W, hd)
    whole = lambda a: pl.BlockSpec(a.shape, lambda i: (0,) * a.ndim)
    rest = (ctx, mod, wq, wk, wv, qg[None, :], kg[None, :]) + tuple(jnp.asarray(t) for t in tables)
    kv_rows = total + ctx.shape[0]
    return pl.pallas_call(
        project_kernel,
        name="project_stage",
        grid=(steps,),
        out_shape=(
            jax.ShapeDtypeStruct((heads, total, hd), BF16),
            jax.ShapeDtypeStruct((kv_rows, 2 * hd), BF16),
        ),
        in_specs=[pl.BlockSpec((ntp // steps, n, d), lambda i: (i, 0, 0))] + [whole(a) for a in rest],
        out_specs=(
            pl.BlockSpec((heads, total, hd), lambda i: (0, 0, 0)),
            pl.BlockSpec((kv_rows, 2 * hd), lambda i: (0, 0)),
        ),
        compiler_params=pltpu.CompilerParams(
            dimension_semantics=("arbitrary",), vmem_limit_bytes=60 * 1024 * 1024
        ),
    )(rows, *rest)


def attend_kernel(
    lift,
    q_in,
    kv_in,
    w_in,
    lat,
    gate,
    out,
    qbuf,
    kvbuf,
    acc,
    top,
    tot,
    osend,
    lsend,
    orecv,
    lrecv,
    orelay,
    lrelay,
    wfull,
    att,
    exch,
    ks,
    kr,
    qs,
    qr,
    ws,
    wr,
    os_,
    or_,
    ls_,
    lr_,
    ts,
    tr,
):
    z, x, y, c = (lax.axis_index(a) for a in ("z", "x", "y", "c"))
    me = y * NC + c
    zp, zm = lax.rem(z + 1, NZ), lax.rem(z + NZ - 1, NZ)
    xp, xm = lax.rem(x + 1, NX), lax.rem(x + NX - 1, NX)
    yp, ym = lax.rem(y + 1, NY), lax.rem(y + NY - 1, NY)
    heads, n, hd = q_in.shape
    n_ctx = kv_in.shape[0] - n
    scale = hd ** (-0.5) * math.log2(math.e)
    raw_lift = lift / hd ** (-0.5)
    t_to = tp_peers(y, c)
    greet([{"z": zp}, {"z": zm}, {"x": xp}, {"x": xm}] + t_to)

    started = []

    def go(*args, **to):
        cp = remote(*args, **to)
        cp.start()
        started.append(cp)
        return cp

    q1 = go(q_in, qbuf.at[1], qs.at[0], qr.at[0], x=xp)
    q2 = go(q_in, qbuf.at[2], qs.at[1], qr.at[1], x=xm)
    k1 = go(kv_in, kvbuf.at[1], ks.at[0], kr.at[0], z=zp)
    k2 = go(kv_in, kvbuf.at[2], ks.at[1], kr.at[1], z=zm)
    w1 = go(w_in, wfull.at[me], ws.at[0], wr.at[0], y=yp)
    w2 = go(w_in, wfull.at[me], ws.at[1], wr.at[1], y=ym)
    w0 = go(w_in, wfull.at[me], ws.at[2], wr.at[2], c=1 - c)

    qbuf[0] = q_in[...]
    kvbuf[0] = kv_in[...]
    wfull[me] = w_in[...]
    acc[...] = jnp.zeros_like(acc)
    tot[...] = jnp.zeros_like(tot)
    top[...] = jnp.full_like(top, -1e30)

    def update(a, h, k, v, add):
        s = lax.dot_general(qbuf[a, h], k, (((1,), (1,)), ((), ())), preferred_element_type=F32)
        if add:
            s = s + add
        wide = s.shape[1] // hd
        old = top[a, h]
        new = jnp.maximum(old, jnp.max(s, axis=1, keepdims=True))
        factor = jnp.exp2((old - new) * scale)
        p = jnp.exp2((s - jnp.concatenate([new] * wide, axis=1)) * scale)
        part = sum((p[:, i * hd : (i + 1) * hd] for i in range(1, wide)), p[:, 0:hd])
        top[a, h] = new
        tot[a, h] = tot[a, h] * factor + part
        acc[a, h] = acc[a, h] * factor + jnp.dot(p.astype(BF16), v, preferred_element_type=F32)

    def run(a0, na, b0, nb):
        def body(i, carry):
            b = b0 + lax.rem(i, nb)
            h = lax.rem(i // nb, heads)
            a = a0 + i // (nb * heads)
            update(a, h, kvbuf[b, 0:n, 0:hd], kvbuf[b, 0:n, hd : 2 * hd], 0.0)
            return carry

        lax.fori_loop(0, na * heads * nb, body, 0)

    def run_ctx(a0, na):
        def body(i, carry):
            kv = jnp.concatenate([kvbuf[b, n : n + n_ctx, :] for b in range(NZ)], axis=0)
            update(a0 + i // heads, lax.rem(i, heads), kv[:, 0:hd], kv[:, hd : 2 * hd], raw_lift)
            return carry

        lax.fori_loop(0, na * heads, body, 0)

    eye = diagonal(hd)
    blocks = n // hd

    def finish(a):
        def body(h, carry):
            total = jnp.sum(tot[a, h], axis=1, keepdims=True)
            osend[a - 1, h] = (acc[a, h] / total).astype(BF16)
            lse = top[a, h] * scale + jnp.log2(total)
            for b in range(blocks):
                row = jnp.sum(jnp.where(eye, lse[b * hd : (b + 1) * hd], 0.0), axis=0, keepdims=True)
                lsend[a - 1, h, b : b + 1, :] = row
            return carry

        lax.fori_loop(0, heads, body, 0)

    run(0, 1, 0, 1)
    q1.wait_recv()
    q2.wait_recv()
    q3 = go(qbuf.at[1, 0], qbuf.at[3, 0], qs.at[2], qr.at[2], x=xp)
    q4 = go(qbuf.at[2, 1], qbuf.at[3, 1], qs.at[3], qr.at[3], x=xm)
    k1.wait_recv()
    k2.wait_recv()
    k3 = go(kvbuf.at[1], kvbuf.at[3], ks.at[2], kr.at[2], z=zp)
    k4 = go(kvbuf.at[2], kvbuf.at[4], ks.at[3], kr.at[3], z=zm)
    run(1, 2, 0, 3)
    q3.wait_recv()
    q4.wait_recv()
    k3.wait_recv()
    k4.wait_recv()
    k5 = go(kvbuf.at[3], kvbuf.at[5], ks.at[4], kr.at[4], z=zp)
    k6 = go(kvbuf.at[4], kvbuf.at[6], ks.at[5], kr.at[5], z=zm)
    run(3, 1, 0, 3)
    run(1, 3, 3, 2)
    k5.wait_recv()
    k6.wait_recv()
    cut = n // 2
    k7 = go(kvbuf.at[5, 0:cut], kvbuf.at[7, 0:cut], ks.at[6], kr.at[6], z=zp)
    k8 = go(kvbuf.at[6, cut : n + n_ctx], kvbuf.at[7, cut : n + n_ctx], ks.at[7], kr.at[7], z=zm)
    run(0, 1, 1, 4)
    w1.wait_recv()
    w2.wait_recv()
    low, high, far = ym * NC + c, yp * NC + c, lax.rem(y + 2, NY) * NC + c
    wh = w_in.shape[0] // 2
    w3 = go(wfull.at[low, 0:wh], wfull.at[low, 0:wh], ws.at[3], wr.at[3], y=yp)
    w4 = go(wfull.at[high, wh : 2 * wh], wfull.at[high, wh : 2 * wh], ws.at[4], wr.at[4], y=ym)
    w5 = go(wfull.at[low], wfull.at[low], ws.at[5], wr.at[5], c=1 - c)
    w6 = go(wfull.at[high], wfull.at[high], ws.at[6], wr.at[6], c=1 - c)
    run(1, 3, 5, 2)
    k7.wait_recv()
    k8.wait_recv()
    run(3, 1, 7, 1)
    run_ctx(3, 1)
    finish(3)
    run(1, 1, 7, 1)
    o3 = go(osend.at[2, 0], orelay.at[0], os_.at[0], or_.at[0], x=xp)
    o4 = go(osend.at[2, 1], orelay.at[1], os_.at[1], or_.at[1], x=xm)
    l3 = go(lsend.at[2, 0], lrelay.at[0], ls_.at[0], lr_.at[0], x=xp)
    l4 = go(lsend.at[2, 1], lrelay.at[1], ls_.at[1], lr_.at[1], x=xm)
    run_ctx(1, 1)
    finish(1)
    run(2, 1, 7, 1)
    o1 = go(osend.at[0], orecv.at[0], os_.at[2], or_.at[2], x=xm)
    l1 = go(lsend.at[0], lrecv.at[0], ls_.at[2], lr_.at[2], x=xm)
    run_ctx(2, 1)
    finish(2)
    run(0, 1, 5, 1)
    o2 = go(osend.at[1], orecv.at[1], os_.at[3], or_.at[3], x=xp)
    l2 = go(lsend.at[1], lrecv.at[1], ls_.at[3], lr_.at[3], x=xp)
    for cp in (o3, o4, l3, l4):
        cp.wait_recv()
    o5 = go(orelay.at[0], orecv.at[2, 0], os_.at[4], or_.at[4], x=xp)
    o6 = go(orelay.at[1], orecv.at[2, 1], os_.at[5], or_.at[5], x=xm)
    l5 = go(lrelay.at[0], lrecv.at[2, 0], ls_.at[4], lr_.at[4], x=xp)
    l6 = go(lrelay.at[1], lrecv.at[2, 1], ls_.at[5], lr_.at[5], x=xm)
    run(0, 1, 6, 2)
    run_ctx(0, 1)
    w3.wait_recv()
    w4.wait_recv()
    w7 = go(wfull.at[far], wfull.at[far], ws.at[7], wr.at[7], c=1 - c)
    for cp in (o1, o2, o5, o6, l1, l2, l5, l6):
        cp.wait_recv()

    for h in range(heads):
        for b in range(blocks):
            at = slice(b * hd, (b + 1) * hd)
            total = jnp.sum(tot[0, h, at, :], axis=1, keepdims=True)
            lse = [top[0, h, at, :] + jnp.log2(total) * (1.0 / scale)]
            for i in range(NX - 1):
                row = jnp.broadcast_to(lrecv[i, h, b : b + 1, :], (hd, hd))
                col = jnp.sum(jnp.where(eye, row, 0.0), axis=1, keepdims=True)
                lse.append(jnp.broadcast_to(col * (1.0 / scale), (hd, hd)))
            best = functools.reduce(jnp.maximum, lse)
            weights = [jnp.exp2((v - best) * scale) for v in lse]
            summed = (acc[0, h, at, :] / total) * weights[0]
            for i in range(NX - 1):
                summed = summed + orecv[i, h, at, :].astype(F32) * weights[i + 1]
            att[at, h * hd : (h + 1) * hd] = (summed / sum(weights[1:], weights[0])).astype(BF16)

    mine = lat.shape[0]
    t_out = []
    for i, to in enumerate(t_to):
        at = pl.multiple_of(tp_index(to, y, c) * mine, mine)
        t_out.append(go(att.at[pl.ds(at, mine), :], exch.at[me], ts.at[i], tr.at[i], **to))
    exch[me] = att[pl.ds(pl.multiple_of(me * mine, mine), mine), :]
    for cp in (w0, w5, w6, w7):
        cp.wait_recv()
    for cp in t_out:
        cp.wait_recv()
    cols = 512
    d = lat.shape[1]
    rows_in = jnp.concatenate([exch[i] for i in range(NTP)], axis=1)
    for j in range(d // cols):
        sl = slice(j * cols, (j + 1) * cols)
        weight = wfull[:, :, sl].reshape(NTP * w_in.shape[0], cols)
        out[:, sl] = jnp.dot(rows_in, weight, preferred_element_type=F32)
    mixed = out[...]
    out[...] = lat[...].astype(F32) + gate[...] * rms(mixed)
    for cp in started:
        cp.wait_send()


def attend_stage(q, kv, w, lat, gate, lift):
    heads, n, hd = q.shape
    kv_rows = kv.shape[0]
    dma = pltpu.SemaphoreType.DMA
    mine, d = lat.shape
    return pl.pallas_call(
        functools.partial(attend_kernel, lift),
        name="attend_stage",
        out_shape=jax.ShapeDtypeStruct((mine, d), F32),
        in_specs=[VMEM_SPEC] * 5,
        out_specs=VMEM_SPEC,
        scratch_shapes=[
            pltpu.VMEM((NX, heads, n, hd), BF16),
            pltpu.VMEM((NZ, kv_rows, 2 * hd), BF16),
            pltpu.VMEM((NX, heads, n, hd), F32),
            pltpu.VMEM((NX, heads, n, hd), F32),
            pltpu.VMEM((NX, heads, n, hd), F32),
            pltpu.VMEM((NX - 1, heads, n, hd), BF16),
            pltpu.VMEM((NX - 1, heads, n // hd, hd), F32),
            pltpu.VMEM((NX - 1, heads, n, hd), BF16),
            pltpu.VMEM((NX - 1, heads, n // hd, hd), F32),
            pltpu.VMEM((heads, n, hd), BF16),
            pltpu.VMEM((heads, n // hd, hd), F32),
            pltpu.VMEM((NTP,) + w.shape, BF16),
            pltpu.VMEM((n, heads * hd), BF16),
            pltpu.VMEM((NTP, mine, heads * hd), BF16),
            dma((8,)),
            dma((8,)),
            dma((4,)),
            dma((4,)),
            dma((8,)),
            dma((8,)),
            dma((6,)),
            dma((6,)),
            dma((6,)),
            dma((6,)),
            dma((NTP - 1,)),
            dma((NTP - 1,)),
        ],
        compiler_params=pltpu.CompilerParams(
            collective_id=1, has_side_effects=True, vmem_limit_bytes=60 * 1024 * 1024
        ),
    )(q, kv, w, lat, gate)


def body(
    latents,
    context,
    cond,
    ctx_cond,
    mod_weight,
    query_weight,
    key_matrix,
    value_matrix,
    out_weight,
    query_gain,
    key_gain,
):
    d = latents.shape[1]
    rows, mod = gather_stage(latents, cond, ctx_cond, mod_weight)
    q, kv = project_stage(
        rows, context, mod, query_weight, key_matrix, value_matrix, query_gain, key_gain
    )
    tokens = latents.shape[0] * NTP * NZ * NX
    lift = math.log(tokens / (2.0 * context.shape[0] * NZ * NX))
    result = attend_stage(q, kv, out_weight, latents, mod[0:1, 2 * d :], lift)
    return result.astype(BF16)


def solution(mesh):
    torus = Mesh(mesh.devices.reshape(NZ, NX, NY, NC), ("z", "x", "y", "c"))
    sp, tp = ("z", "x"), ("y", "c")
    placed = (
        P(sp + tp, None),
        P(sp, None),
        P(sp),
        P(sp),
        P(sp, tp),
        P(None, tp),
        P(None, tp),
        P(None, tp),
        P(tp, None),
        P(),
        P(),
    )
    return jax.shard_map(body, mesh=torus, in_specs=placed, out_specs=P(sp + tp, None), check_vma=False)
```

```python
import functools
import math

import jax
import jax.numpy as jnp
import numpy as np
from jax import lax
from jax.experimental import pallas as pl
from jax.experimental.pallas import tpu as pltpu
from jax.sharding import Mesh
from jax.sharding import PartitionSpec as P

MESH_ID = pl.DeviceIdType.MESH
GRID_W = 64
NORM_EPS = 1e-06
ROPE_BASE = 10000.0
NZ, NX, NY, NC = 8, 4, 4, 2
NTP = NY * NC
BF16, F32 = jnp.bfloat16, jnp.float32
VMEM_SPEC = pl.BlockSpec(memory_space=pltpu.VMEM)


def remote(src, dst, send_sem, recv_sem, **to):
    return pltpu.make_async_remote_copy(
        src_ref=src,
        dst_ref=dst,
        send_sem=send_sem,
        recv_sem=recv_sem,
        device_id=to,
        device_id_type=MESH_ID,
    )


class View:
    def __init__(self, ref, index=None):
        self.ref, self.index = ref, index

    def __getitem__(self, index):
        return View(self.ref, index)


def make(*args, **to):
    return remote(*(a.ref.at[a.index] if isinstance(a, View) else a for a in args), **to)


def greet(peers):
    barrier = pltpu.get_barrier_semaphore()
    for peer in peers:
        pl.semaphore_signal(barrier, inc=1, device_id=peer, device_id_type=MESH_ID)
    pl.semaphore_wait(barrier, len(peers))


def tp_peers(y, c):
    peers = [{"c": 1 - c}]
    for dy in range(1, NY):
        for dc in range(NC):
            peers.append({"y": lax.rem(y + dy, NY), "c": lax.rem(c + dc, NC)})
    return peers


def tp_index(peer, y, c):
    return peer.get("y", y) * NC + peer["c"]


def diagonal(n):
    return lax.broadcasted_iota(jnp.int32, (n, n), 0) == lax.broadcasted_iota(jnp.int32, (n, n), 1)


def rope_tables(row_tokens, freqs):
    c = freqs // 4
    inv = (ROPE_BASE ** (-np.arange(c, dtype=np.float32) / np.float32(c))).astype(np.float32)

    def table(count, lanes_from):
        angles = np.arange(count, dtype=np.float32)[:, None] * inv[None, :]
        cos, sin = np.cos(angles), np.sin(angles)
        out_c = np.zeros((count, freqs), np.float32)
        out_s = np.zeros((count, freqs), np.float32)
        out_c[:, lanes_from : lanes_from + 2 * c] = np.concatenate([cos, cos], 1)
        out_s[:, lanes_from : lanes_from + 2 * c] = np.concatenate([-sin, sin], 1)
        return out_c, out_s

    return table(row_tokens, 0) + table(GRID_W, freqs // 2)


def rms(v):
    return v * lax.rsqrt(jnp.mean(v * v, axis=-1, keepdims=True) + NORM_EPS)


def block_kernel(
    lift,
    lat,
    ctx,
    cond,
    ctx_cond,
    mod_weight,
    qg,
    kg,
    row_c,
    row_s,
    col_c,
    col_s,
    wq_hbm,
    wk_hbm,
    wv_hbm,
    w_hbm,
    out,
    rows,
    normed,
    mod,
    part,
    px,
    pt,
    zbuf,
    xbuf,
    tbuf,
    wq,
    wkv,
    qbuf,
    kvbuf,
    cbuf,
    acc,
    top,
    tot,
    osend,
    lsend,
    orecv,
    lrecv,
    orelay,
    lrelay,
    wfull,
    att,
    exch,
    mixed,
    loc,
    rs,
    rr,
    zs,
    zr,
    xs,
    xr,
    ms,
    mr,
    ks,
    kr,
    qs,
    qr,
    ws,
    wr,
    os_,
    or_,
    ls_,
    lr_,
    ts,
    tr,
):
    z, x, y, c = (lax.axis_index(a) for a in ("z", "x", "y", "c"))
    me = y * NC + c
    zp, zm = lax.rem(z + 1, NZ), lax.rem(z + NZ - 1, NZ)
    xp, xm = lax.rem(x + 1, NX), lax.rem(x + NX - 1, NX)
    yp, ym = lax.rem(y + 1, NY), lax.rem(y + NY - 1, NY)
    low, high, far = ym * NC + c, yp * NC + c, lax.rem(y + 2, NY) * NC + c
    mine, d = lat.shape
    heads, n, hd = qbuf.shape[1:]
    n_ctx = ctx.shape[0]
    scale = hd ** (-0.5) * math.log2(math.e)
    raw_lift = lift / hd ** (-0.5)

    fetch = [
        pltpu.make_async_copy(wk_hbm, wkv.at[:, 0:hd], loc.at[0]),
        pltpu.make_async_copy(wv_hbm, wkv.at[:, hd : 2 * hd], loc.at[1]),
        pltpu.make_async_copy(wq_hbm, wq, loc.at[2]),
        pltpu.make_async_copy(w_hbm, wfull.at[me], loc.at[3]),
    ]
    for cp in fetch:
        cp.start()

    z_to = [{"z": lax.rem(z + i, NZ)} for i in range(1, NZ)]
    x_to = [{"x": lax.rem(x + i, NX)} for i in range(1, NX)]
    t_to = tp_peers(y, c)
    greet(z_to + x_to + t_to)

    started = []

    def go(*args, **to):
        cp = functools.partial(make, *args, **to)
        cp().start()
        started.append(cp)
        return cp

    def got(copies):
        for cp in copies:
            cp().wait_recv()

    rh = mine // 2
    rpiece = (pl.ds(0, rh), pl.ds(rh, rh))

    def r_to(src, row, p, i, **to):
        return go(src, View(rows)[row, rpiece[p]], View(rs)[i], View(rr)[i], **to)

    up = [r_to(View(lat)[rpiece[p]], me, p, p, y=yp) for p in (0, 1)]
    down = [r_to(View(lat)[rpiece[p]], me, p, 2 + p, y=ym) for p in (1, 0)]
    across = [go(lat, View(rows)[me], View(rs)[6], View(rr)[6], c=1 - c)]

    eye_in = diagonal(cond.shape[1])
    for r, ref in enumerate((cond, ctx_cond)):
        v = ref[...]
        v = v * jax.nn.sigmoid(v)
        column = jnp.sum(jnp.where(eye_in, jnp.broadcast_to(v, eye_in.shape), 0.0), axis=1, keepdims=True)
        part[r : r + 1, :] = jnp.sum(column * mod_weight[...], axis=0, keepdims=True)
    z_out = [go(part, View(zbuf)[z], View(zs)[i], View(zr)[i], **to) for i, to in enumerate(z_to)]
    zbuf[z] = part[...]
    rows[me] = lat[...]
    acc[...] = jnp.zeros_like(acc)
    tot[...] = jnp.zeros_like(tot)
    top[...] = jnp.full_like(top, -1e30)
    got(z_out)
    px[...] = sum((zbuf[i] for i in range(1, NZ)), zbuf[0])
    x_out = [go(px, View(xbuf)[x], View(xs)[i], View(xr)[i], **to) for i, to in enumerate(x_to)]
    xbuf[x] = px[...]
    got([up[0], down[0]])
    up2 = r_to(View(rows)[low, rpiece[0]], low, 0, 4, y=yp)
    down2 = r_to(View(rows)[high, rpiece[1]], high, 1, 5, y=ym)
    got(x_out)
    pt[...] = sum((xbuf[i] for i in range(1, NX)), xbuf[0])
    m_out = [go(pt, View(tbuf)[me], View(ms)[i], View(mr)[i], **to) for i, to in enumerate(t_to)]
    tbuf[me] = pt[...]
    got([up[1], down[1]])
    across.append(go(View(rows)[low], View(rows)[low], View(rs)[7], View(rr)[7], c=1 - c))
    across.append(go(View(rows)[high], View(rows)[high], View(rs)[8], View(rr)[8], c=1 - c))
    got([up2, down2])
    across.append(go(View(rows)[far], View(rows)[far], View(rs)[9], View(rr)[9], c=1 - c))
    for cp in fetch:
        cp.wait()

    wh = w_hbm.shape[0] // 2
    wpiece = (pl.ds(0, wh), pl.ds(wh, wh))

    def w_to(row, p, i, **to):
        piece = View(wfull)[row, wpiece[p]]
        return go(piece, piece, View(ws)[i], View(wr)[i], **to)

    w1 = [w_to(me, p, p, y=yp) for p in (0, 1)]
    w2 = [w_to(me, p, 2 + p, y=ym) for p in (1, 0)]
    w0 = go(View(wfull)[me], View(wfull)[me], View(ws)[8], View(wr)[8], c=1 - c)
    got(m_out)
    w = part.shape[1]
    for i in range(NTP):
        mod[:, i * w : (i + 1) * w] = tbuf[i]
    got(across)

    cut = n // 2
    kpiece = (pl.ds(0, cut), pl.ds(cut, cut + n_ctx))

    def k_to(src, slot, p, **to):
        i = 2 * (slot - 1) + p
        return go(View(kvbuf)[src, kpiece[p]], View(kvbuf)[slot, kpiece[p]], View(ks)[i], View(kr)[i], **to)

    def q_to(src, slot, h, **to):
        i = 2 * (slot - 1) + h
        return go(View(qbuf)[src, h], View(qbuf)[slot, h], View(qs)[i], View(qr)[i], **to)

    def modulated(v, r):
        v = rms(v.astype(F32))
        return (v * (1.0 + mod[r : r + 1, d : 2 * d]) + mod[r : r + 1, 0:d]).astype(BF16)

    groups = cut // GRID_W
    first = (z * NX + x) * (n // GRID_W)
    lane = lax.broadcasted_iota(jnp.int32, (cut, hd), 1)
    early = lax.rem(lane, hd // 2) < hd // 4

    def table(row_table, col_table, i):
        at = [first + i * groups + g for g in range(groups)]
        return jnp.concatenate([row_table[pl.ds(t, 1), :] + col_table[...] for t in at], axis=0)

    def turned(v, i):
        other = jnp.where(early, pltpu.roll(v, hd - hd // 4, 1), pltpu.roll(v, hd // 4, 1))
        return (v * table(row_c, col_c, i) + other * table(row_s, col_s, i)).astype(BF16)

    k1, k2 = [], []
    per = NTP // 2
    for i in range(2):
        for g in range(per):
            normed[i * per + g] = modulated(rows[i * per + g], 0)
        a = normed[i * per : (i + 1) * per].reshape(cut, d)
        kv = jnp.dot(a, wkv[...], preferred_element_type=F32)
        at = slice(i * cut, (i + 1) * cut)
        kvbuf[0, at, 0:hd] = turned(rms(kv[:, 0:hd]) * kg[...], i)
        kvbuf[0, at, hd : 2 * hd] = kv[:, hd : 2 * hd].astype(BF16)
        if i == 1:
            kv = jnp.dot(modulated(ctx[...], 1), wkv[...], preferred_element_type=F32)
            kvbuf[0, n : n + n_ctx, 0:hd] = (rms(kv[:, 0:hd]) * kg[...]).astype(BF16)
            kvbuf[0, n : n + n_ctx, hd : 2 * hd] = kv[:, hd : 2 * hd].astype(BF16)
        k1.append(k_to(0, 1, i, z=zp))
        k2.append(k_to(0, 2, i, z=zm))
    for i in range(2):
        a = normed[i * per : (i + 1) * per].reshape(cut, d)
        q = jnp.dot(a, wq[...], preferred_element_type=F32)
        for h in range(heads):
            at = slice(i * cut, (i + 1) * cut)
            qbuf[0, h, at, :] = turned(rms(q[:, h * hd : (h + 1) * hd]) * qg[...], i)
    q1 = [q_to(0, 1, h, x=xp) for h in (0, 1)]
    q2 = [q_to(0, 2, h, x=xm) for h in (1, 0)]

    def scores(a, h, k):
        return lax.dot_general(qbuf[a, h], k, (((1,), (1,)), ((), ())), preferred_element_type=F32)

    def update(a, h, s, v):
        wide = s.shape[1] // hd
        old = top[a, h]
        new = jnp.maximum(old, jnp.max(s, axis=1, keepdims=True))
        factor = jnp.exp2((old - new) * scale)
        p = jnp.exp2((s - jnp.concatenate([new] * wide, axis=1)) * scale)
        some = sum((p[:, i * hd : (i + 1) * hd] for i in range(1, wide)), p[:, 0:hd])
        top[a, h] = new
        tot[a, h] = tot[a, h] * factor + some
        acc[a, h] = acc[a, h] * factor + jnp.dot(p.astype(BF16), v, preferred_element_type=F32)

    def tile(a, slots, tail=False):
        more = [cbuf[...]] if tail else []
        m = n * len(slots)
        k = jnp.concatenate([kvbuf[b, 0:n, 0:hd] for b in slots] + [e[:, 0:hd] for e in more], axis=0)
        v = jnp.concatenate([kvbuf[b, 0:n, hd : 2 * hd] for b in slots] + [e[:, hd : 2 * hd] for e in more], axis=0)
        found = [scores(a, h, k) for h in range(heads)]
        for h in range(heads):
            s = found[h]
            if tail:
                s = jnp.concatenate([s[:, 0:m], s[:, m:] + raw_lift], axis=1)
            update(a, h, s, v)

    eye = diagonal(hd)
    blocks = n // hd

    def join(a, h, others, o_to, l_to):
        for b in range(blocks):
            at = pl.ds(b * hd, hd)
            total = jnp.sum(tot[a, h, at, :], axis=1, keepdims=True)
            value = acc[a, h, at, :] / total
            lse = top[a, h, at, :] * scale + jnp.log2(total)
            if others:
                lses, values = [lse], [value]
                for o_ref, l_ref in others:
                    row = jnp.broadcast_to(l_ref[b : b + 1, :], (hd, hd))
                    col = jnp.sum(jnp.where(eye, row, 0.0), axis=1, keepdims=True)
                    lses.append(jnp.broadcast_to(col, (hd, hd)))
                    values.append(o_ref[at, :].astype(F32))
                best = functools.reduce(jnp.maximum, lses)
                weights = [jnp.exp2(v - best) for v in lses]
                total = sum(weights[1:], weights[0])
                value = sum((w * v for w, v in zip(weights[1:], values[1:])), weights[0] * values[0]) / total
                lse = best + jnp.log2(total)
            o_to(b, value.astype(BF16))
            if l_to is not None:
                l_to[b : b + 1, :] = jnp.sum(jnp.where(eye, lse, 0.0), axis=0, keepdims=True)

    def finish(a, h, others=()):
        def put(b, value):
            osend[a - 1, h, b * hd : (b + 1) * hd, :] = value

        join(a, h, others, put, lsend.at[a - 1, h])

    def o_go(a, h, to_o, to_l, i, **to):
        ls = go(View(lsend)[a - 1, h], to_l, View(ls_)[i], View(lr_)[i], **to)
        return [ls, go(View(osend)[a - 1, h], to_o, View(os_)[i], View(or_)[i], **to)]

    k3, k4, k5, k6, k7, q34, w34 = [], [], [], [], [], [], []
    got([k1[0], k2[0]])
    k3.append(k_to(1, 3, 0, z=zp))
    k4.append(k_to(2, 4, 0, z=zm))
    got([k1[1], k2[1]])
    k3.append(k_to(1, 3, 1, z=zp))
    k4.append(k_to(2, 4, 1, z=zm))
    got([q1[0], q2[0]])
    q34.append(q_to(1, 3, 0, x=xp))
    q34.append(q_to(2, 3, 1, x=xm))
    got([q1[1], q2[1]])

    def one(j, carry):
        @pl.when(j == 1)
        def _():
            got([k3[0], k4[0]])
            k5.append(k_to(3, 5, 0, z=zp))
            k6.append(k_to(4, 6, 0, z=zm))

        @pl.when(j == 3)
        def _():
            got([k3[1], k4[1]])
            k5.append(k_to(3, 5, 1, z=zp))
            k6.append(k_to(4, 6, 1, z=zm))
            got(q34)

        tile(jnp.where(j == 2, 0, jnp.where(j == 3, 3, j + 1)), (0, 1, 2))
        return carry

    lax.fori_loop(0, 4, one, 0)

    def two(j, carry):
        @pl.when(j == 0)
        def _():
            got([k5[0], k6[0]])
            k7.append(k_to(5, 7, 0, z=zp))
            got([w1[0], w2[0]])
            w34.append(w_to(low, 0, 4, y=yp))
            w34.append(w_to(high, 1, 5, y=ym))

        @pl.when(j == 2)
        def _():
            got([k5[1], k6[1]])
            k7.append(k_to(6, 7, 1, z=zm))

        tile(jnp.where(j == 3, 0, j + 1), (3, 4))
        return carry

    lax.fori_loop(0, 4, two, 0)
    got(k7)
    for b in range(NZ):
        cbuf[b * n_ctx : (b + 1) * n_ctx, :] = kvbuf[b, n : n + n_ctx, :]

    late = (5, 6, 7)
    tile(3, late, True)
    finish(3, 0)
    finish(3, 1)
    far0 = o_go(3, 0, View(orelay)[0], View(lrelay)[0], 0, x=xp)
    far1 = o_go(3, 1, View(orelay)[1], View(lrelay)[1], 1, x=xm)

    def near(a, carry):
        tile(a, late, True)
        return carry

    lax.fori_loop(1, 3, near, 0)
    finish(1, 0)
    finish(2, 1)
    pure0 = o_go(1, 0, View(orecv)[1, 0], View(lrecv)[1, 0], 2, x=xm)
    pure1 = o_go(2, 1, View(orecv)[0, 1], View(lrecv)[0, 1], 3, x=xp)
    got([w1[1], w2[1]])
    w5 = go(View(wfull)[low], View(wfull)[low], View(ws)[6], View(wr)[6], c=1 - c)
    w6 = go(View(wfull)[high], View(wfull)[high], View(ws)[7], View(wr)[7], c=1 - c)
    got(far0 + far1)
    finish(2, 0, [(orelay.at[0], lrelay.at[0])])
    finish(1, 1, [(orelay.at[1], lrelay.at[1])])
    both0 = o_go(2, 0, View(orecv)[0, 0], View(lrecv)[0, 0], 4, x=xp)
    both1 = o_go(1, 1, View(orecv)[1, 1], View(lrecv)[1, 1], 5, x=xm)
    tile(0, late, True)
    got(w34)
    w7 = go(View(wfull)[far], View(wfull)[far], View(ws)[9], View(wr)[9], c=1 - c)
    got(pure0 + pure1 + both0 + both1)

    for h in range(heads):

        def put(b, value, h=h):
            att[b * hd : (b + 1) * hd, h * hd : (h + 1) * hd] = value

        join(0, h, [(orecv.at[i, h], lrecv.at[i, h]) for i in range(2)], put, None)

    t_out = [None] * len(t_to)
    for i in (3, 4, 1, 2, 5, 6, 0):
        at = pl.multiple_of(tp_index(t_to[i], y, c) * mine, mine)
        t_out[i] = go(View(att)[pl.ds(at, mine), :], View(exch)[me], View(ts)[i], View(tr)[i], **t_to[i])
    exch[me] = att[pl.ds(pl.multiple_of(me * mine, mine), mine), :]

    def add(source, fresh=False):
        product = jnp.dot(exch[source], wfull[source], preferred_element_type=F32)
        mixed[...] = product if fresh else mixed[...] + product

    def came(i):
        got([t_out[i]])
        back = {1: 5, 2: 6, 5: 1, 6: 2}.get(i, i)
        add(tp_index(t_to[back], y, c))

    add(me, True)
    got([w0])
    came(0)
    got([w5, w6])
    for i in (1, 2, 5, 6):
        came(i)
    got([w7])
    for i in (3, 4):
        came(i)
    out[...] = (lat[...].astype(F32) + mod[0:1, 2 * d : 3 * d] * rms(mixed[...])).astype(BF16)
    for cp in started:
        cp().wait_send()


def body(
    latents,
    context,
    cond,
    ctx_cond,
    mod_weight,
    query_weight,
    key_matrix,
    value_matrix,
    out_weight,
    query_gain,
    key_gain,
):
    mine, d = latents.shape
    n_ctx = context.shape[0]
    hd = query_gain.shape[0]
    heads = query_weight.shape[1] // hd
    n = mine * NTP
    kv_rows = n + n_ctx
    cols = mod_weight.shape[1]
    tokens = n * NZ * NX
    lift = math.log(tokens / (2.0 * n_ctx * NZ * NX))
    tables = [jnp.asarray(t) for t in rope_tables(tokens // GRID_W, hd)]
    dma = pltpu.SemaphoreType.DMA
    pairs = [s for count in (10, NZ - 1, NX - 1, NTP - 1, 14, 6, 10, 6, 6, NTP - 1) for s in (dma((count,)),) * 2]
    return pl.pallas_call(
        functools.partial(block_kernel, lift),
        name="block_stage",
        out_shape=jax.ShapeDtypeStruct((mine, d), BF16),
        in_specs=[VMEM_SPEC] * 11 + [pl.BlockSpec(memory_space=pl.ANY)] * 4,
        out_specs=VMEM_SPEC,
        scratch_shapes=[
            pltpu.VMEM((NTP, mine, d), BF16),
            pltpu.VMEM((NTP, mine, d), BF16),
            pltpu.VMEM((2, NTP * cols), F32),
            pltpu.VMEM((2, cols), F32),
            pltpu.VMEM((2, cols), F32),
            pltpu.VMEM((2, cols), F32),
            pltpu.VMEM((NZ, 2, cols), F32),
            pltpu.VMEM((NX, 2, cols), F32),
            pltpu.VMEM((NTP, 2, cols), F32),
            pltpu.VMEM(query_weight.shape, BF16),
            pltpu.VMEM((d, 2 * hd), BF16),
            pltpu.VMEM((NX, heads, n, hd), BF16),
            pltpu.VMEM((NZ, kv_rows, 2 * hd), BF16),
            pltpu.VMEM((NZ * n_ctx, 2 * hd), BF16),
            pltpu.VMEM((NX, heads, n, hd), F32),
            pltpu.VMEM((NX, heads, n, hd), F32),
            pltpu.VMEM((NX, heads, n, hd), F32),
            pltpu.VMEM((NX - 1, heads, n, hd), BF16),
            pltpu.VMEM((NX - 1, heads, n // hd, hd), F32),
            pltpu.VMEM((2, heads, n, hd), BF16),
            pltpu.VMEM((2, heads, n // hd, hd), F32),
            pltpu.VMEM((2, n, hd), BF16),
            pltpu.VMEM((2, n // hd, hd), F32),
            pltpu.VMEM((NTP,) + out_weight.shape, BF16),
            pltpu.VMEM((n, heads * hd), BF16),
            pltpu.VMEM((NTP, mine, heads * hd), BF16),
            pltpu.VMEM((mine, d), F32),
            dma((4,)),
        ]
        + pairs,
        compiler_params=pltpu.CompilerParams(
            collective_id=0, has_side_effects=True, vmem_limit_bytes=62 * 1024 * 1024
        ),
    )(
        latents,
        context,
        cond[None, :],
        ctx_cond[None, :],
        mod_weight,
        query_gain[None, :],
        key_gain[None, :],
        *tables,
        query_weight,
        key_matrix,
        value_matrix,
        out_weight,
    )


def solution(mesh):
    torus = Mesh(mesh.devices.reshape(NZ, NX, NY, NC), ("z", "x", "y", "c"))
    sp, tp = ("z", "x"), ("y", "c")
    placed = (
        P(sp + tp, None),
        P(sp, None),
        P(sp),
        P(sp),
        P(sp, tp),
        P(None, tp),
        P(None, tp),
        P(None, tp),
        P(tp, None),
        P(),
        P(),
    )
    return jax.shard_map(body, mesh=torus, in_specs=placed, out_specs=P(sp + tp, None), check_vma=False)
```

```python
import functools
import math

import jax
import jax.numpy as jnp
import numpy as np
from jax import lax
from jax.experimental import pallas as pl
from jax.experimental.pallas import tpu as pltpu
from jax.sharding import Mesh
from jax.sharding import PartitionSpec as P

MESH_ID = pl.DeviceIdType.MESH
GRID_W = 64
NORM_EPS = 1e-06
ROPE_BASE = 10000.0
NZ, NX, NY, NC = 8, 4, 4, 2
NTP = NY * NC
BF16, F32 = jnp.bfloat16, jnp.float32
VMEM_SPEC = pl.BlockSpec(memory_space=pltpu.VMEM)


def remote(src, dst, send_sem, recv_sem, **to):
    return pltpu.make_async_remote_copy(
        src_ref=src,
        dst_ref=dst,
        send_sem=send_sem,
        recv_sem=recv_sem,
        device_id=to,
        device_id_type=MESH_ID,
    )


class View:
    def __init__(self, ref, index=None):
        self.ref, self.index = ref, index

    def __getitem__(self, index):
        return View(self.ref, index)


def make(*args, **to):
    return remote(*(a.ref.at[a.index] if isinstance(a, View) else a for a in args), **to)


def greet(peers):
    barrier = pltpu.get_barrier_semaphore()
    for peer in peers:
        pl.semaphore_signal(barrier, inc=1, device_id=peer, device_id_type=MESH_ID)
    return functools.partial(pl.semaphore_wait, barrier, len(peers))


def tp_peers(y, c):
    peers = [{"c": 1 - c}]
    for dy in range(1, NY):
        for dc in range(NC):
            peers.append({"y": lax.rem(y + dy, NY), "c": lax.rem(c + dc, NC)})
    return peers


def tp_index(peer, y, c):
    return peer.get("y", y) * NC + peer["c"]


def diagonal(n):
    return lax.broadcasted_iota(jnp.int32, (n, n), 0) == lax.broadcasted_iota(jnp.int32, (n, n), 1)


def rope_tables(row_tokens, freqs):
    c = freqs // 4
    inv = (ROPE_BASE ** (-np.arange(c, dtype=np.float32) / np.float32(c))).astype(np.float32)

    def table(count, lanes_from):
        angles = np.arange(count, dtype=np.float32)[:, None] * inv[None, :]
        cos, sin = np.cos(angles), np.sin(angles)
        out_c = np.zeros((count, freqs), np.float32)
        out_s = np.zeros((count, freqs), np.float32)
        out_c[:, lanes_from : lanes_from + 2 * c] = np.concatenate([cos, cos], 1)
        out_s[:, lanes_from : lanes_from + 2 * c] = np.concatenate([-sin, sin], 1)
        return out_c, out_s

    return table(row_tokens, 0) + table(GRID_W, freqs // 2)


def rms(v):
    return v * lax.rsqrt(jnp.mean(v * v, axis=-1, keepdims=True) + NORM_EPS)


def block_kernel(
    lift,
    *refs,
):
    (
        lat_hbm,
        ctx_hbm,
        cond_hbm,
        ctx_cond_hbm,
        mod_weight_hbm,
        qg_hbm,
        kg_hbm,
        row_c_hbm,
        row_s_hbm,
        col_c_hbm,
        col_s_hbm,
        wq_hbm,
        wk_hbm,
        wv_hbm,
        w_hbm,
        out,
        *refs,
    ) = refs
    (lat, ctx, cond, ctx_cond, mod_weight, qg, kg, row_c, row_s, col_c, col_s, *refs) = refs
    (
    rows,
    normed,
    mod,
    part,
    px,
    pt,
    zbuf,
    xbuf,
    tbuf,
    wq,
    wkv,
    qbuf,
    kvbuf,
    cbuf,
    acc,
    top,
    tot,
    osend,
    lsend,
    orecv,
    lrecv,
    orelay,
    lrelay,
    wfull,
    att,
    exch,
    mixed,
    loc,
    rs,
    rr,
    zs,
    zr,
    xs,
    xr,
    ms,
    mr,
    ks,
    kr,
    qs,
    qr,
    ws,
    wr,
    os_,
    or_,
    ls_,
    lr_,
    ts,
    tr,
    ) = refs
    z, x, y, c = (lax.axis_index(a) for a in ("z", "x", "y", "c"))
    me = y * NC + c
    zp, zm = lax.rem(z + 1, NZ), lax.rem(z + NZ - 1, NZ)
    xp, xm = lax.rem(x + 1, NX), lax.rem(x + NX - 1, NX)
    yp, ym = lax.rem(y + 1, NY), lax.rem(y + NY - 1, NY)
    low, high, far = ym * NC + c, yp * NC + c, lax.rem(y + 2, NY) * NC + c
    mine, d = lat.shape
    heads, n, hd = qbuf.shape[1:]
    n_ctx = ctx.shape[0]
    scale = hd ** (-0.5) * math.log2(math.e)
    raw_lift = lift / hd ** (-0.5)


    z_to = [{"z": lax.rem(z + i, NZ)} for i in range(1, NZ)]
    x_to = [{"x": lax.rem(x + i, NX)} for i in range(1, NX)]
    t_to = tp_peers(y, c)
    greeted = greet(z_to + x_to + t_to)

    fetches = (
        (lat_hbm, lat),
        (mod_weight_hbm, mod_weight),
        (cond_hbm, cond),
        (ctx_cond_hbm, ctx_cond),
        (wk_hbm, wkv.at[:, 0:hd]),
        (wv_hbm, wkv.at[:, hd : 2 * hd]),
        (ctx_hbm, ctx),
        (row_c_hbm, row_c),
        (row_s_hbm, row_s),
        (col_c_hbm, col_c),
        (col_s_hbm, col_s),
        (qg_hbm, qg),
        (kg_hbm, kg),
        (wq_hbm, wq),
        (w_hbm, wfull.at[me]),
    )
    fetch = [pltpu.make_async_copy(src, dst, loc.at[i]) for i, (src, dst) in enumerate(fetches)]
    for cp in fetch:
        cp.start()
    for cp in fetch[0:4]:
        cp.wait()

    started = []

    def go(*args, **to):
        cp = functools.partial(make, *args, **to)
        cp().start()
        started.append(cp)
        return cp

    def got(copies):
        for cp in copies:
            cp().wait_recv()

    rh = mine // 2
    rpiece = (pl.ds(0, rh), pl.ds(rh, rh))

    def r_to(src, row, p, i, **to):
        return go(src, View(rows)[row, rpiece[p]], View(rs)[i], View(rr)[i], **to)

    eye_in = diagonal(cond.shape[1])
    for r, ref in enumerate((cond, ctx_cond)):
        v = ref[...]
        v = v * jax.nn.sigmoid(v)
        column = jnp.sum(jnp.where(eye_in, jnp.broadcast_to(v, eye_in.shape), 0.0), axis=1, keepdims=True)
        part[r : r + 1, :] = jnp.sum(column * mod_weight[...], axis=0, keepdims=True)
    rows[me] = lat[...]
    acc[...] = jnp.zeros_like(acc)
    tot[...] = jnp.zeros_like(tot)
    top[...] = jnp.full_like(top, -1e30)
    greeted()

    z_out = [None] * len(z_to)
    for i in (3, 2, 4, 1, 5, 0, 6):
        z_out[i] = go(part, View(zbuf)[z], View(zs)[i], View(zr)[i], **z_to[i])
    up = [r_to(View(lat)[rpiece[p]], me, p, p, y=yp) for p in (0, 1)]
    down = [r_to(View(lat)[rpiece[p]], me, p, 2 + p, y=ym) for p in (1, 0)]
    across = [go(lat, View(rows)[me], View(rs)[6], View(rr)[6], c=1 - c)]
    zbuf[z] = part[...]
    got(z_out)
    px[...] = sum((zbuf[i] for i in range(1, NZ)), zbuf[0])
    x_out = [go(px, View(xbuf)[x], View(xs)[i], View(xr)[i], **to) for i, to in enumerate(x_to)]
    xbuf[x] = px[...]
    got([up[0], down[0]])
    up2 = r_to(View(rows)[low, rpiece[0]], low, 0, 4, y=yp)
    down2 = r_to(View(rows)[high, rpiece[1]], high, 1, 5, y=ym)
    got(x_out)
    pt[...] = sum((xbuf[i] for i in range(1, NX)), xbuf[0])
    m_out = [go(pt, View(tbuf)[me], View(ms)[i], View(mr)[i], **to) for i, to in enumerate(t_to)]
    tbuf[me] = pt[...]
    got([up[1], down[1]])
    across.append(go(View(rows)[low], View(rows)[low], View(rs)[7], View(rr)[7], c=1 - c))
    across.append(go(View(rows)[high], View(rows)[high], View(rs)[8], View(rr)[8], c=1 - c))
    got([up2, down2])
    across.append(go(View(rows)[far], View(rows)[far], View(rs)[9], View(rr)[9], c=1 - c))
    for cp in fetch[4:]:
        cp.wait()

    wh = w_hbm.shape[0] // 2
    wpiece = (pl.ds(0, wh), pl.ds(wh, wh))

    def w_to(row, p, i, **to):
        piece = View(wfull)[row, wpiece[p]]
        return go(piece, piece, View(ws)[i], View(wr)[i], **to)

    w1 = [w_to(me, p, p, y=yp) for p in (0, 1)]
    w2 = [w_to(me, p, 2 + p, y=ym) for p in (1, 0)]
    w0 = go(View(wfull)[me], View(wfull)[me], View(ws)[8], View(wr)[8], c=1 - c)
    got(m_out)
    w = part.shape[1]
    for i in range(NTP):
        mod[:, i * w : (i + 1) * w] = tbuf[i]
    got(across)

    cut = n // 2
    quarter = n // 4
    kpiece = [pl.ds(p * quarter, quarter) for p in range(3)] + [pl.ds(3 * quarter, quarter + n_ctx)]
    plus, minus = (0, 1, 2, 3), (2, 3, 0, 1)

    def k_to(src, slot, p, **to):
        i = 4 * (slot - 1) + p
        return go(View(kvbuf)[src, kpiece[p]], View(kvbuf)[slot, kpiece[p]], View(ks)[i], View(kr)[i], **to)

    def q_to(src, slot, h, **to):
        i = 2 * (slot - 1) + h
        return go(View(qbuf)[src, h], View(qbuf)[slot, h], View(qs)[i], View(qr)[i], **to)

    def modulated(v, r):
        v = rms(v.astype(F32))
        return (v * (1.0 + mod[r : r + 1, d : 2 * d]) + mod[r : r + 1, 0:d]).astype(BF16)

    groups = cut // GRID_W
    first = (z * NX + x) * (n // GRID_W)
    lane = lax.broadcasted_iota(jnp.int32, (cut, hd), 1)
    early = lax.rem(lane, hd // 2) < hd // 4

    def table(row_table, col_table, i):
        at = [first + i * groups + g for g in range(groups)]
        return jnp.concatenate([row_table[pl.ds(t, 1), :] + col_table[...] for t in at], axis=0)

    def turned(v, i):
        other = jnp.where(early, pltpu.roll(v, hd - hd // 4, 1), pltpu.roll(v, hd // 4, 1))
        return (v * table(row_c, col_c, i) + other * table(row_s, col_s, i)).astype(BF16)

    k1, k2 = {}, {}
    per = NTP // 2
    for i in range(2):
        for g in range(per):
            normed[i * per + g] = modulated(rows[i * per + g], 0)
        a = normed[i * per : (i + 1) * per].reshape(cut, d)
        kv = jnp.dot(a, wkv[...], preferred_element_type=F32)
        at = slice(i * cut, (i + 1) * cut)
        kvbuf[0, at, 0:hd] = turned(rms(kv[:, 0:hd]) * kg[...], i)
        kvbuf[0, at, hd : 2 * hd] = kv[:, hd : 2 * hd].astype(BF16)
        if i == 1:
            kv = jnp.dot(modulated(ctx[...], 1), wkv[...], preferred_element_type=F32)
            kvbuf[0, n : n + n_ctx, 0:hd] = (rms(kv[:, 0:hd]) * kg[...]).astype(BF16)
            kvbuf[0, n : n + n_ctx, hd : 2 * hd] = kv[:, hd : 2 * hd].astype(BF16)
        for p in plus[2 * i : 2 * i + 2]:
            k1[p] = k_to(0, 1, p, z=zp)
        if i == 1:
            for p in minus:
                k2[p] = k_to(0, 2, p, z=zm)
    for i in range(2):
        a = normed[i * per : (i + 1) * per].reshape(cut, d)
        q = jnp.dot(a, wq[...], preferred_element_type=F32)
        for h in range(heads):
            at = slice(i * cut, (i + 1) * cut)
            qbuf[0, h, at, :] = turned(rms(q[:, h * hd : (h + 1) * hd]) * qg[...], i)
    q1 = [q_to(0, 1, h, x=xp) for h in (0, 1)]
    q2 = [q_to(0, 2, h, x=xm) for h in (1, 0)]

    def scores(a, h, k):
        return lax.dot_general(qbuf[a, h], k, (((1,), (1,)), ((), ())), preferred_element_type=F32)

    def update(a, h, s, v):
        wide = s.shape[1] // hd
        old = top[a, h]
        new = jnp.maximum(old, jnp.max(s, axis=1, keepdims=True))
        factor = jnp.exp2((old - new) * scale)
        p = jnp.exp2((s - jnp.concatenate([new] * wide, axis=1)) * scale)
        some = sum((p[:, i * hd : (i + 1) * hd] for i in range(1, wide)), p[:, 0:hd])
        top[a, h] = new
        tot[a, h] = tot[a, h] * factor + some
        acc[a, h] = acc[a, h] * factor + jnp.dot(p.astype(BF16), v, preferred_element_type=F32)

    def tile(works, slots, tail=False):
        more = [cbuf[...]] if tail else []
        m = n * len(slots)
        k = jnp.concatenate([kvbuf[b, 0:n, 0:hd] for b in slots] + [e[:, 0:hd] for e in more], axis=0)
        v = jnp.concatenate([kvbuf[b, 0:n, hd : 2 * hd] for b in slots] + [e[:, hd : 2 * hd] for e in more], axis=0)
        found = [scores(a, h, k) for a, h in works]
        for (a, h), s in zip(works, found):
            if tail:
                s = jnp.concatenate([s[:, 0:m], s[:, m:] + raw_lift], axis=1)
            update(a, h, s, v)

    def both_heads(a):
        return [(a, h) for h in range(heads)]

    eye = diagonal(hd)
    blocks = n // hd

    parts = 2
    pb = blocks // parts

    def join(a, h, t, others, o_to, l_to):
        for b in range(pb):
            at = pl.ds((t * pb + b) * hd, hd)
            here = pl.ds(b * hd, hd)
            total = jnp.sum(tot[a, h, at, :], axis=1, keepdims=True)
            value = acc[a, h, at, :] / total
            lse = top[a, h, at, :] * scale + jnp.log2(total)
            if others:
                lses, values = [lse], [value]
                for o_ref, l_ref in others:
                    row = jnp.broadcast_to(l_ref[b : b + 1, :], (hd, hd))
                    col = jnp.sum(jnp.where(eye, row, 0.0), axis=1, keepdims=True)
                    lses.append(jnp.broadcast_to(col, (hd, hd)))
                    values.append(o_ref[here, :].astype(F32))
                best = functools.reduce(jnp.maximum, lses)
                weights = [jnp.exp2(v - best) for v in lses]
                total = sum(weights[1:], weights[0])
                value = sum((w * v for w, v in zip(weights[1:], values[1:])), weights[0] * values[0]) / total
                lse = best + jnp.log2(total)
            o_to(b, value.astype(BF16))
            if l_to is not None:
                l_to[b : b + 1, :] = jnp.sum(jnp.where(eye, lse, 0.0), axis=0, keepdims=True)

    def finish(a, h, t, others=()):
        def put(b, value):
            osend[a - 1, h, t, b * hd : (b + 1) * hd, :] = value

        join(a, h, t, others, put, lsend.at[a - 1, h, t])

    def o_go(a, h, t, to_o, to_l, i, **to):
        i = 2 * i + t
        ls = go(View(lsend)[a - 1, h, t], to_l, View(ls_)[i], View(lr_)[i], **to)
        return [ls, go(View(osend)[a - 1, h, t], to_o, View(os_)[i], View(or_)[i], **to)]

    ring = {1: k1, 2: k2}
    for slot in range(3, NZ):
        ring[slot] = {}

    def pass_on(hop, i):
        src_p, src_m = 2 * hop - 1, 2 * hop
        got([ring[src_p][plus[i]], ring[src_m][minus[i]]])
        last = hop == 3
        ring[src_p + 2][plus[i]] = k_to(src_p, src_p + 2, plus[i], z=zp)
        to_slot = src_p + 2 if last else src_m + 2
        ring[to_slot][minus[i]] = k_to(src_m, to_slot, minus[i], z=zm)

    q34, w34 = [], []
    tile(both_heads(0), (0,))
    for i in range(4):
        pass_on(1, i)
    got([q1[0], q2[0]])
    q34.append(q_to(1, 3, 0, x=xp))
    q34.append(q_to(2, 3, 1, x=xm))
    tile(both_heads(0), (1, 2))
    got([q1[1], q2[1]])

    def one(a, carry):
        @pl.when(a == 1)
        def _():
            pass_on(2, 0)

        @pl.when(a == 2)
        def _():
            pass_on(2, 1)

        @pl.when(a == 3)
        def _():
            pass_on(2, 2)
            pass_on(2, 3)
            got(q34)

        tile(both_heads(a), (0, 1, 2))
        return carry

    lax.fori_loop(1, 4, one, 0)

    def two(a, carry):
        @pl.when(a == 1)
        def _():
            pass_on(3, 0)

        @pl.when(a == 2)
        def _():
            pass_on(3, 1)
            got([w1[0], w2[0]])
            w34.append(w_to(low, 0, 4, y=yp))
            w34.append(w_to(high, 1, 5, y=ym))

        tile(both_heads(a), (3, 4))
        return carry

    lax.fori_loop(1, 4, two, 0)
    got([ring[5][p] for p in plus[2:]] + [ring[6][p] for p in minus[2:]])
    tile(both_heads(3), (5, 6))
    got([ring[7][p] for p in range(4)])
    for b in range(NZ):
        cbuf[b * n_ctx : (b + 1) * n_ctx, :] = kvbuf[b, n : n + n_ctx, :]

    late = (5, 6, 7)
    tile(both_heads(3), (7,), True)
    far0, far1, pure0, pure1, both0, both1 = [], [], [], [], [], []
    for t in range(parts):
        finish(3, 0, t)
        finish(3, 1, t)
        far0.append(o_go(3, 0, t, View(orelay)[0, t], View(lrelay)[0, t], 0, x=xp))
        far1.append(o_go(3, 1, t, View(orelay)[1, t], View(lrelay)[1, t], 1, x=xm))

    def near(i, carry):
        tile([(1 + i, 0), (2 - i, 1)], late, True)

        @pl.when(i == 0)
        def _():
            for t in range(parts):
                finish(1, 0, t)
                finish(2, 1, t)
                pure0.append(o_go(1, 0, t, View(orecv)[1, 0, t], View(lrecv)[1, 0, t], 2, x=xm))
                pure1.append(o_go(2, 1, t, View(orecv)[0, 1, t], View(lrecv)[0, 1, t], 3, x=xp))

        return carry

    lax.fori_loop(0, 2, near, 0)
    got([w1[1], w2[1]])
    w5 = go(View(wfull)[low], View(wfull)[low], View(ws)[6], View(wr)[6], c=1 - c)
    w6 = go(View(wfull)[high], View(wfull)[high], View(ws)[7], View(wr)[7], c=1 - c)
    for t in range(parts):
        got(far0[t] + far1[t])
        finish(2, 0, t, [(orelay.at[0, t], lrelay.at[0, t])])
        finish(1, 1, t, [(orelay.at[1, t], lrelay.at[1, t])])
        both0.append(o_go(2, 0, t, View(orecv)[0, 0, t], View(lrecv)[0, 0, t], 4, x=xp))
        both1.append(o_go(1, 1, t, View(orecv)[1, 1, t], View(lrecv)[1, 1, t], 5, x=xm))
    tile(both_heads(0), (3, 4))
    tile(both_heads(0), late, True)
    got(w34)
    w7 = go(View(wfull)[far], View(wfull)[far], View(ws)[9], View(wr)[9], c=1 - c)

    for t in range(parts):
        got(pure0[t] + pure1[t] + both0[t] + both1[t])
        for h in range(heads):

            def put(b, value, h=h, t=t):
                att[(t * pb + b) * hd : (t * pb + b + 1) * hd, h * hd : (h + 1) * hd] = value

            join(0, h, t, [(orecv.at[i, h, t], lrecv.at[i, h, t]) for i in range(2)], put, None)

    t_out = [None] * len(t_to)
    for i in (3, 4, 1, 2, 5, 6, 0):
        at = pl.multiple_of(tp_index(t_to[i], y, c) * mine, mine)
        t_out[i] = go(View(att)[pl.ds(at, mine), :], View(exch)[me], View(ts)[i], View(tr)[i], **t_to[i])
    exch[me] = att[pl.ds(pl.multiple_of(me * mine, mine), mine), :]

    def add(source, fresh=False):
        product = jnp.dot(exch[source], wfull[source], preferred_element_type=F32)
        mixed[...] = product if fresh else mixed[...] + product

    def came(i):
        got([t_out[i]])
        back = {1: 5, 2: 6, 5: 1, 6: 2}.get(i, i)
        add(tp_index(t_to[back], y, c))

    add(me, True)
    got([w0])
    came(0)
    got([w5, w6])
    for i in (1, 2, 5, 6):
        came(i)
    got([w7])
    for i in (3, 4):
        came(i)
    out[...] = (lat[...].astype(F32) + mod[0:1, 2 * d : 3 * d] * rms(mixed[...])).astype(BF16)
    for cp in started:
        cp().wait_send()


def body(
    latents,
    context,
    cond,
    ctx_cond,
    mod_weight,
    query_weight,
    key_matrix,
    value_matrix,
    out_weight,
    query_gain,
    key_gain,
):
    mine, d = latents.shape
    n_ctx = context.shape[0]
    hd = query_gain.shape[0]
    heads = query_weight.shape[1] // hd
    n = mine * NTP
    kv_rows = n + n_ctx
    cols = mod_weight.shape[1]
    tokens = n * NZ * NX
    lift = math.log(tokens / (2.0 * n_ctx * NZ * NX))
    tables = [jnp.asarray(t) for t in rope_tables(tokens // GRID_W, hd)]
    dma = pltpu.SemaphoreType.DMA
    pairs = [s for count in (10, NZ - 1, NX - 1, NTP - 1, 28, 6, 10, 12, 12, NTP - 1) for s in (dma((count,)),) * 2]
    inputs = (
        latents,
        context,
        cond[None, :],
        ctx_cond[None, :],
        mod_weight,
        query_gain[None, :],
        key_gain[None, :],
        *tables,
        query_weight,
        key_matrix,
        value_matrix,
        out_weight,
    )
    return pl.pallas_call(
        functools.partial(block_kernel, lift),
        name="block_stage",
        out_shape=pltpu.VMEM((mine, d), BF16),
        in_specs=[pl.BlockSpec(memory_space=pl.ANY)] * len(inputs),
        out_specs=VMEM_SPEC,
        scratch_shapes=[pltpu.VMEM(a.shape, a.dtype) for a in inputs[:11]]
        + [
            pltpu.VMEM((NTP, mine, d), BF16),
            pltpu.VMEM((NTP, mine, d), BF16),
            pltpu.VMEM((2, NTP * cols), F32),
            pltpu.VMEM((2, cols), F32),
            pltpu.VMEM((2, cols), F32),
            pltpu.VMEM((2, cols), F32),
            pltpu.VMEM((NZ, 2, cols), F32),
            pltpu.VMEM((NX, 2, cols), F32),
            pltpu.VMEM((NTP, 2, cols), F32),
            pltpu.VMEM(query_weight.shape, BF16),
            pltpu.VMEM((d, 2 * hd), BF16),
            pltpu.VMEM((NX, heads, n, hd), BF16),
            pltpu.VMEM((NZ, kv_rows, 2 * hd), BF16),
            pltpu.VMEM((NZ * n_ctx, 2 * hd), BF16),
            pltpu.VMEM((NX, heads, n, hd), F32),
            pltpu.VMEM((NX, heads, n, hd), F32),
            pltpu.VMEM((NX, heads, n, hd), F32),
            pltpu.VMEM((NX - 1, heads, 2, n // 2, hd), BF16),
            pltpu.VMEM((NX - 1, heads, 2, n // hd // 2, hd), F32),
            pltpu.VMEM((2, heads, 2, n // 2, hd), BF16),
            pltpu.VMEM((2, heads, 2, n // hd // 2, hd), F32),
            pltpu.VMEM((2, 2, n // 2, hd), BF16),
            pltpu.VMEM((2, 2, n // hd // 2, hd), F32),
            pltpu.VMEM((NTP,) + out_weight.shape, BF16),
            pltpu.VMEM((n, heads * hd), BF16),
            pltpu.VMEM((NTP, mine, heads * hd), BF16),
            pltpu.VMEM((mine, d), F32),
            dma((15,)),
        ]
        + pairs,
        compiler_params=pltpu.CompilerParams(
            collective_id=0, has_side_effects=True, vmem_limit_bytes=62 * 1024 * 1024
        ),
    )(*inputs)


def solution(mesh):
    torus = Mesh(mesh.devices.reshape(NZ, NX, NY, NC), ("z", "x", "y", "c"))
    sp, tp = ("z", "x"), ("y", "c")
    placed = (
        P(sp + tp, None),
        P(sp, None),
        P(sp),
        P(sp),
        P(sp, tp),
        P(None, tp),
        P(None, tp),
        P(None, tp),
        P(tp, None),
        P(),
        P(),
    )
    return jax.shard_map(body, mesh=torus, in_specs=placed, out_specs=P(sp + tp, None), check_vma=False)
```

```python
import functools
import math

import jax
import jax.numpy as jnp
import numpy as np
from jax import lax
from jax.experimental import pallas as pl
from jax.experimental.pallas import tpu as pltpu
from jax.sharding import Mesh
from jax.sharding import PartitionSpec as P

MESH_ID = pl.DeviceIdType.MESH
GRID_W = 64
NORM_EPS = 1e-06
ROPE_BASE = 10000.0
NZ, NX, NY, NC = 8, 4, 4, 2
NTP = NY * NC
BF16, F32 = jnp.bfloat16, jnp.float32
VMEM_SPEC = pl.BlockSpec(memory_space=pltpu.VMEM)


def remote(src, dst, send_sem, recv_sem, **to):
    return pltpu.make_async_remote_copy(
        src_ref=src,
        dst_ref=dst,
        send_sem=send_sem,
        recv_sem=recv_sem,
        device_id=to,
        device_id_type=MESH_ID,
    )


class View:
    def __init__(self, ref, index=None):
        self.ref, self.index = ref, index

    def __getitem__(self, index):
        return View(self.ref, index)


def make(*args, **to):
    return remote(*(a.ref.at[a.index] if isinstance(a, View) else a for a in args), **to)


def greet(peers):
    barrier = pltpu.get_barrier_semaphore()
    for peer in peers:
        pl.semaphore_signal(barrier, inc=1, device_id=peer, device_id_type=MESH_ID)
    return functools.partial(pl.semaphore_wait, barrier, len(peers))


def tp_peers(y, c):
    peers = [{"c": 1 - c}]
    for dy in range(1, NY):
        for dc in range(NC):
            peers.append({"y": lax.rem(y + dy, NY), "c": lax.rem(c + dc, NC)})
    return peers


def tp_index(peer, y, c):
    return peer.get("y", y) * NC + peer["c"]


def diagonal(n):
    return lax.broadcasted_iota(jnp.int32, (n, n), 0) == lax.broadcasted_iota(jnp.int32, (n, n), 1)


def rope_tables(row_tokens, freqs):
    c = freqs // 4
    inv = (ROPE_BASE ** (-np.arange(c, dtype=np.float32) / np.float32(c))).astype(np.float32)

    def table(count, lanes_from):
        angles = np.arange(count, dtype=np.float32)[:, None] * inv[None, :]
        cos, sin = np.cos(angles), np.sin(angles)
        out_c = np.zeros((count, freqs), np.float32)
        out_s = np.zeros((count, freqs), np.float32)
        out_c[:, lanes_from : lanes_from + 2 * c] = np.concatenate([cos, cos], 1)
        out_s[:, lanes_from : lanes_from + 2 * c] = np.concatenate([-sin, sin], 1)
        return out_c, out_s

    return table(row_tokens, 0) + table(GRID_W, freqs // 2)


def rms(v):
    return v * lax.rsqrt(jnp.mean(v * v, axis=-1, keepdims=True) + NORM_EPS)


def block_kernel(
    lift,
    *refs,
):
    (
        lat_hbm,
        ctx_hbm,
        cond_hbm,
        ctx_cond_hbm,
        mod_weight_hbm,
        qg_hbm,
        kg_hbm,
        row_c_hbm,
        row_s_hbm,
        col_c_hbm,
        col_s_hbm,
        wq_hbm,
        wk_hbm,
        wv_hbm,
        w_hbm,
        out,
        *refs,
    ) = refs
    (lat, ctx, cond, ctx_cond, mod_weight, qg, kg, row_c, row_s, col_c, col_s, *refs) = refs
    (
    rows,
    normed,
    mod,
    part,
    px,
    pt,
    zbuf,
    xbuf,
    tbuf,
    wq,
    wkv,
    qbuf,
    kvbuf,
    cbuf,
    acc,
    top,
    tot,
    osend,
    lsend,
    orecv,
    lrecv,
    orelay,
    lrelay,
    wfull,
    att,
    exch,
    mixed,
    loc,
    rs,
    rr,
    zs,
    zr,
    xs,
    xr,
    ms,
    mr,
    ks,
    kr,
    qs,
    qr,
    ws,
    wr,
    os_,
    or_,
    ls_,
    lr_,
    ts,
    tr,
    ) = refs
    z, x, y, c = (lax.axis_index(a) for a in ("z", "x", "y", "c"))
    me = y * NC + c
    zp, zm = lax.rem(z + 1, NZ), lax.rem(z + NZ - 1, NZ)
    xp, xm = lax.rem(x + 1, NX), lax.rem(x + NX - 1, NX)
    yp, ym = lax.rem(y + 1, NY), lax.rem(y + NY - 1, NY)
    low, high, far = ym * NC + c, yp * NC + c, lax.rem(y + 2, NY) * NC + c
    mine, d = lat.shape
    heads, n, hd = qbuf.shape[1:]
    n_ctx = ctx.shape[0]
    scale = hd ** (-0.5) * math.log2(math.e)
    raw_lift = lift / hd ** (-0.5)


    z_to = [{"z": lax.rem(z + i, NZ)} for i in range(1, NZ)]
    x_to = [{"x": lax.rem(x + i, NX)} for i in range(1, NX)]
    t_to = tp_peers(y, c)
    greeted = greet(z_to + x_to + t_to)

    fetches = (
        (lat_hbm, lat),
        (mod_weight_hbm, mod_weight),
        (cond_hbm, cond),
        (ctx_cond_hbm, ctx_cond),
        (wk_hbm, wkv.at[:, 0:hd]),
        (wv_hbm, wkv.at[:, hd : 2 * hd]),
        (ctx_hbm, ctx),
        (row_c_hbm, row_c),
        (row_s_hbm, row_s),
        (col_c_hbm, col_c),
        (col_s_hbm, col_s),
        (qg_hbm, qg),
        (kg_hbm, kg),
        (wq_hbm, wq),
        (w_hbm, wfull.at[me]),
    )
    fetch = [pltpu.make_async_copy(src, dst, loc.at[i]) for i, (src, dst) in enumerate(fetches)]
    for cp in fetch:
        cp.start()
    for cp in fetch[0:4]:
        cp.wait()

    def go(src, dst, sems, i, **to):
        make(src, dst, View(sems[0])[0], View(sems[1])[i], **to).start()

    def got(view, sems, i):
        make(view, view, View(sems[0])[0], View(sems[1])[i], c=1 - c).wait_recv()

    def gone(view, sems):
        make(view, view, View(sems[0])[0], View(sems[1])[0], c=1 - c).wait_send()

    r_, z_, x_, m_, k_, q_, w_, o_, l_, t_ = (
        (rs, rr), (zs, zr), (xs, xr), (ms, mr), (ks, kr), (qs, qr), (ws, wr), (os_, or_), (ls_, lr_), (ts, tr),
    )

    rh = mine // 2
    rpiece = (pl.ds(0, rh), pl.ds(rh, rh))

    def r_to(src, row, p, i, **to):
        go(src, View(rows)[row, rpiece[p]], r_, i, **to)

    eye_in = diagonal(cond.shape[1])
    for r, ref in enumerate((cond, ctx_cond)):
        v = ref[...]
        v = v * jax.nn.sigmoid(v)
        column = jnp.sum(jnp.where(eye_in, jnp.broadcast_to(v, eye_in.shape), 0.0), axis=1, keepdims=True)
        part[r : r + 1, :] = jnp.sum(column * mod_weight[...], axis=0, keepdims=True)
    rows[me] = lat[...]
    acc[...] = jnp.zeros_like(acc)
    tot[...] = jnp.zeros_like(tot)
    top[...] = jnp.full_like(top, -1e30)
    greeted()

    for i in (3, 2, 4, 1, 5, 0, 6):
        go(part, View(zbuf)[z], z_, 0, **z_to[i])
    for i in range(2):
        r_to(View(lat)[rpiece[i]], me, i, i, y=yp)
        r_to(View(lat)[rpiece[1 - i]], me, 1 - i, i, y=ym)
    go(lat, View(rows)[me], r_, 3, c=1 - c)
    zbuf[z] = part[...]
    got(View(zbuf)[0 : NZ - 1], z_, 0)
    px[...] = sum((zbuf[i] for i in range(1, NZ)), zbuf[0])
    for to in x_to:
        go(px, View(xbuf)[x], x_, 0, **to)
    xbuf[x] = px[...]
    got(View(rows)[0], r_, 0)
    r_to(View(rows)[low, rpiece[0]], low, 0, 2, y=yp)
    r_to(View(rows)[high, rpiece[1]], high, 1, 2, y=ym)
    got(View(xbuf)[0 : NX - 1], x_, 0)
    pt[...] = sum((xbuf[i] for i in range(1, NX)), xbuf[0])
    for to in t_to:
        go(pt, View(tbuf)[me], m_, 0, **to)
    tbuf[me] = pt[...]
    got(View(rows)[0], r_, 1)
    go(View(rows)[low], View(rows)[low], r_, 3, c=1 - c)
    go(View(rows)[high], View(rows)[high], r_, 3, c=1 - c)
    got(View(rows)[0], r_, 2)
    go(View(rows)[far], View(rows)[far], r_, 3, c=1 - c)
    for cp in fetch[4:]:
        cp.wait()

    wh = w_hbm.shape[0] // 2
    wpiece = (pl.ds(0, wh), pl.ds(wh, wh))

    def w_to(row, p, i, **to):
        piece = View(wfull)[row, wpiece[p]]
        go(piece, piece, w_, i, **to)

    for i in range(2):
        w_to(me, i, i, y=yp)
        w_to(me, 1 - i, i, y=ym)
    go(View(wfull)[me], View(wfull)[me], w_, 3, c=1 - c)
    got(View(tbuf)[0 : NTP - 1], m_, 0)
    w = part.shape[1]
    for i in range(NTP):
        mod[:, i * w : (i + 1) * w] = tbuf[i]
    got(View(rows)[0:4], r_, 3)

    cut = n // 2
    quarter = n // 4
    kpiece = [pl.ds(p * quarter, quarter) for p in range(3)] + [pl.ds(3 * quarter, quarter + n_ctx)]
    plus, minus = (0, 1, 2, 3), (2, 3, 0, 1)

    def k_to(src, slot, p, **to):
        order = plus if slot % 2 else minus
        i = 12 if slot == NZ - 1 else 4 * ((slot - 1) // 2) + order.index(p)
        go(View(kvbuf)[src, kpiece[p]], View(kvbuf)[slot, kpiece[p]], k_, i, **to)

    def k_got(hop, i):
        count = kpiece[plus[i]].size + kpiece[minus[i]].size
        got(View(kvbuf)[0, 0:count], k_, 4 * (hop - 1) + i)

    def q_to(src, slot, h, i, **to):
        go(View(qbuf)[src, h], View(qbuf)[slot, h], q_, i, **to)

    def modulated(v, r):
        v = rms(v.astype(F32))
        return (v * (1.0 + mod[r : r + 1, d : 2 * d]) + mod[r : r + 1, 0:d]).astype(BF16)

    groups = cut // GRID_W
    first = (z * NX + x) * (n // GRID_W)
    lane = lax.broadcasted_iota(jnp.int32, (cut, hd), 1)
    early = lax.rem(lane, hd // 2) < hd // 4

    def table(row_table, col_table, i):
        at = [first + i * groups + g for g in range(groups)]
        return jnp.concatenate([row_table[pl.ds(t, 1), :] + col_table[...] for t in at], axis=0)

    def turned(v, i):
        other = jnp.where(early, pltpu.roll(v, hd - hd // 4, 1), pltpu.roll(v, hd // 4, 1))
        return (v * table(row_c, col_c, i) + other * table(row_s, col_s, i)).astype(BF16)

    per = NTP // 2
    for i in range(2):
        for g in range(per):
            normed[i * per + g] = modulated(rows[i * per + g], 0)
        a = normed[i * per : (i + 1) * per].reshape(cut, d)
        kv = jnp.dot(a, wkv[...], preferred_element_type=F32)
        at = slice(i * cut, (i + 1) * cut)
        kvbuf[0, at, 0:hd] = turned(rms(kv[:, 0:hd]) * kg[...], i)
        kvbuf[0, at, hd : 2 * hd] = kv[:, hd : 2 * hd].astype(BF16)
        if i == 1:
            kv = jnp.dot(modulated(ctx[...], 1), wkv[...], preferred_element_type=F32)
            kvbuf[0, n : n + n_ctx, 0:hd] = (rms(kv[:, 0:hd]) * kg[...]).astype(BF16)
            kvbuf[0, n : n + n_ctx, hd : 2 * hd] = kv[:, hd : 2 * hd].astype(BF16)
        for p in plus[2 * i : 2 * i + 2]:
            k_to(0, 1, p, z=zp)
        if i == 1:
            for p in minus:
                k_to(0, 2, p, z=zm)
    for i in range(2):
        a = normed[i * per : (i + 1) * per].reshape(cut, d)
        q = jnp.dot(a, wq[...], preferred_element_type=F32)
        for h in range(heads):
            at = slice(i * cut, (i + 1) * cut)
            qbuf[0, h, at, :] = turned(rms(q[:, h * hd : (h + 1) * hd]) * qg[...], i)
    for i in range(2):
        q_to(0, 1, i, i, x=xp)
        q_to(0, 2, 1 - i, i, x=xm)

    def scores(a, h, k):
        return lax.dot_general(qbuf[a, h], k, (((1,), (1,)), ((), ())), preferred_element_type=F32)

    def update(a, h, s, v):
        wide = s.shape[1] // hd
        old = top[a, h]
        new = jnp.maximum(old, jnp.max(s, axis=1, keepdims=True))
        factor = jnp.exp2((old - new) * scale)
        p = jnp.exp2((s - jnp.concatenate([new] * wide, axis=1)) * scale)
        some = sum((p[:, i * hd : (i + 1) * hd] for i in range(1, wide)), p[:, 0:hd])
        top[a, h] = new
        tot[a, h] = tot[a, h] * factor + some
        acc[a, h] = acc[a, h] * factor + jnp.dot(p.astype(BF16), v, preferred_element_type=F32)

    def tile(works, slots, tail=False):
        spans = [b if isinstance(b, tuple) else (b, 0, n) for b in slots]
        m = sum(hi - lo for _, lo, hi in spans)

        def take(lane):
            at = slice(lane, lane + hd)
            return jnp.concatenate([kvbuf[b, lo:hi, at] for b, lo, hi in spans] + ([cbuf[:, at]] if tail else []), axis=0)

        k, v = take(0), take(hd)
        found = [scores(a, h, k) for a, h in works]
        for (a, h), s in zip(works, found):
            if tail:
                s = jnp.concatenate([s[:, 0:m], s[:, m:] + raw_lift], axis=1)
            update(a, h, s, v)

    def both_heads(a):
        return [(a, h) for h in range(heads)]

    eye = diagonal(hd)
    blocks = n // hd

    parts = 2
    pb = blocks // parts

    def join(a, h, t, others, o_to, l_to):
        for b in range(pb):
            at = pl.ds((t * pb + b) * hd, hd)
            here = pl.ds(b * hd, hd)
            total = jnp.sum(tot[a, h, at, :], axis=1, keepdims=True)
            value = acc[a, h, at, :] / total
            lse = top[a, h, at, :] * scale + jnp.log2(total)
            if others:
                lses, values = [lse], [value]
                for o_ref, l_ref in others:
                    row = jnp.broadcast_to(l_ref[b : b + 1, :], (hd, hd))
                    col = jnp.sum(jnp.where(eye, row, 0.0), axis=1, keepdims=True)
                    lses.append(jnp.broadcast_to(col, (hd, hd)))
                    values.append(o_ref[here, :].astype(F32))
                best = functools.reduce(jnp.maximum, lses)
                weights = [jnp.exp2(v - best) for v in lses]
                total = sum(weights[1:], weights[0])
                value = sum((w * v for w, v in zip(weights[1:], values[1:])), weights[0] * values[0]) / total
                lse = best + jnp.log2(total)
            o_to(b, value.astype(BF16))
            if l_to is not None:
                l_to[b : b + 1, :] = jnp.sum(jnp.where(eye, lse, 0.0), axis=0, keepdims=True)

    def finish(a, h, t, others=()):
        def put(b, value):
            osend[a - 1, h, t, b * hd : (b + 1) * hd, :] = value

        join(a, h, t, others, put, lsend.at[a - 1, h, t])

    def o_go(a, h, t, to_o, to_l, i, **to):
        go(View(lsend)[a - 1, h, t], to_l, l_, i, **to)
        go(View(osend)[a - 1, h, t], to_o, o_, i, **to)

    def o_got(o_view, l_view, i):
        got(l_view, l_, i)
        got(o_view, o_, i)

    def pass_on(hop, i):
        src_p, src_m = 2 * hop - 1, 2 * hop
        k_got(hop, i)
        k_to(src_p, src_p + 2, plus[i], z=zp)
        k_to(src_m, src_p + 2 if hop == 3 else src_m + 2, minus[i], z=zm)

    tile(both_heads(0), (0,))
    pass_on(1, 0)
    pass_on(1, 1)
    tile(both_heads(0), ((1, 0, cut), (2, cut, n)))
    pass_on(1, 2)
    pass_on(1, 3)
    got(View(qbuf)[1], q_, 0)
    q_to(1, 3, 0, 2, x=xp)
    q_to(2, 3, 1, 2, x=xm)
    tile(both_heads(0), ((1, cut, n), (2, 0, cut)))
    got(View(qbuf)[1], q_, 1)

    def one(a, carry):
        @pl.when(a == 1)
        def _():
            pass_on(2, 0)

        @pl.when(a == 2)
        def _():
            pass_on(2, 1)

        @pl.when(a == 3)
        def _():
            pass_on(2, 2)
            pass_on(2, 3)
            got(View(qbuf)[1], q_, 2)

        tile(both_heads(a), (0, 1, 2))
        return carry

    lax.fori_loop(1, 4, one, 0)

    def two(a, carry):
        @pl.when(a == 1)
        def _():
            pass_on(3, 0)

        @pl.when(a == 2)
        def _():
            pass_on(3, 1)
            got(View(wfull)[0], w_, 0)
            w_to(low, 0, 2, y=yp)
            w_to(high, 1, 2, y=ym)

        tile(both_heads(a), (3, 4))
        return carry

    lax.fori_loop(1, 4, two, 0)
    k_got(3, 2)
    k_got(3, 3)
    tile(both_heads(3), (5, 6))
    got(View(kvbuf)[0], k_, 12)
    for b in range(NZ):
        cbuf[b * n_ctx : (b + 1) * n_ctx, :] = kvbuf[b, n : n + n_ctx, :]

    late = (5, 6, 7)
    tile(both_heads(3), (7,), True)
    for t in range(parts):
        finish(3, 0, t)
        finish(3, 1, t)
        o_go(3, 0, t, View(orelay)[0, t], View(lrelay)[0, t], t, x=xp)
        o_go(3, 1, t, View(orelay)[1, t], View(lrelay)[1, t], t, x=xm)

    def near(i, carry):
        tile([(1 + i, 0), (2 - i, 1)], late, True)

        @pl.when(i == 0)
        def _():
            for t in range(parts):
                finish(1, 0, t)
                finish(2, 1, t)
                o_go(1, 0, t, View(orecv)[1, 0, t], View(lrecv)[1, 0, t], parts + t, x=xm)
                o_go(2, 1, t, View(orecv)[0, 1, t], View(lrecv)[0, 1, t], parts + t, x=xp)

        return carry

    lax.fori_loop(0, 2, near, 0)
    got(View(wfull)[0], w_, 1)
    go(View(wfull)[low], View(wfull)[low], w_, 4, c=1 - c)
    go(View(wfull)[high], View(wfull)[high], w_, 4, c=1 - c)
    for t in range(parts):
        o_got(View(orelay)[0], View(lrelay)[0], t)
        finish(2, 0, t, [(orelay.at[0, t], lrelay.at[0, t])])
        finish(1, 1, t, [(orelay.at[1, t], lrelay.at[1, t])])
        o_go(2, 0, t, View(orecv)[0, 0, t], View(lrecv)[0, 0, t], parts + t, x=xp)
        o_go(1, 1, t, View(orecv)[1, 1, t], View(lrecv)[1, 1, t], parts + t, x=xm)
    tile(both_heads(0), (3, 4))
    tile(both_heads(0), late, True)
    got(View(wfull)[0], w_, 2)
    go(View(wfull)[far], View(wfull)[far], w_, 5, c=1 - c)

    for t in range(parts):
        o_got(View(orecv)[0], View(lrecv)[0], parts + t)
        for h in range(heads):

            def put(b, value, h=h, t=t):
                att[(t * pb + b) * hd : (t * pb + b + 1) * hd, h * hd : (h + 1) * hd] = value

            join(0, h, t, [(orecv.at[i, h, t], lrecv.at[i, h, t]) for i in range(2)], put, None)

    for i in (3, 4, 1, 2, 5, 6, 0):
        at = pl.multiple_of(tp_index(t_to[i], y, c) * mine, mine)
        go(View(att)[pl.ds(at, mine), :], View(exch)[me], t_, i, **t_to[i])
    exch[me] = att[pl.ds(pl.multiple_of(me * mine, mine), mine), :]

    def add(source, fresh=False):
        product = jnp.dot(exch[source], wfull[source], preferred_element_type=F32)
        mixed[...] = product if fresh else mixed[...] + product

    def came(i):
        got(View(exch)[0], t_, i)
        back = {1: 5, 2: 6, 5: 1, 6: 2}.get(i, i)
        add(tp_index(t_to[back], y, c))

    add(me, True)
    got(View(wfull)[0], w_, 3)
    came(0)
    got(View(wfull)[0:2], w_, 4)
    for i in (1, 2, 5, 6):
        came(i)
    got(View(wfull)[0], w_, 5)
    for i in (3, 4):
        came(i)
    out[...] = (lat[...].astype(F32) + mod[0:1, 2 * d : 3 * d] * rms(mixed[...])).astype(BF16)
    sent = (
        (View(rows)[0 : NTP - 1], r_),
        (View(zbuf)[0 : NZ - 1], z_),
        (View(xbuf)[0 : NX - 1], x_),
        (View(tbuf)[0 : NTP - 1], m_),
        (View(kvbuf)[1:NZ], k_),
        (View(qbuf)[1:NX], q_),
        (View(wfull)[0 : NTP - 1], w_),
        (osend, o_),
        (lsend, l_),
        (View(exch)[0 : NTP - 1], t_),
    )
    for view, sems in sent:
        gone(view, sems)


def body(
    latents,
    context,
    cond,
    ctx_cond,
    mod_weight,
    query_weight,
    key_matrix,
    value_matrix,
    out_weight,
    query_gain,
    key_gain,
):
    mine, d = latents.shape
    n_ctx = context.shape[0]
    hd = query_gain.shape[0]
    heads = query_weight.shape[1] // hd
    n = mine * NTP
    kv_rows = n + n_ctx
    cols = mod_weight.shape[1]
    tokens = n * NZ * NX
    lift = math.log(tokens / (2.0 * n_ctx * NZ * NX))
    tables = [jnp.asarray(t) for t in rope_tables(tokens // GRID_W, hd)]
    dma = pltpu.SemaphoreType.DMA
    kinds = (4, 1, 1, 1, 13, 3, 6, 4, 4, NTP - 1)
    pairs = [dma((c,)) for count in kinds for c in (1, count)]
    inputs = (
        latents,
        context,
        cond[None, :],
        ctx_cond[None, :],
        mod_weight,
        query_gain[None, :],
        key_gain[None, :],
        *tables,
        query_weight,
        key_matrix,
        value_matrix,
        out_weight,
    )
    return pl.pallas_call(
        functools.partial(block_kernel, lift),
        name="block_stage",
        out_shape=pltpu.VMEM((mine, d), BF16),
        in_specs=[pl.BlockSpec(memory_space=pl.ANY)] * len(inputs),
        out_specs=VMEM_SPEC,
        scratch_shapes=[pltpu.VMEM(a.shape, a.dtype) for a in inputs[:11]]
        + [
            pltpu.VMEM((NTP, mine, d), BF16),
            pltpu.VMEM((NTP, mine, d), BF16),
            pltpu.VMEM((2, NTP * cols), F32),
            pltpu.VMEM((2, cols), F32),
            pltpu.VMEM((2, cols), F32),
            pltpu.VMEM((2, cols), F32),
            pltpu.VMEM((NZ, 2, cols), F32),
            pltpu.VMEM((NX, 2, cols), F32),
            pltpu.VMEM((NTP, 2, cols), F32),
            pltpu.VMEM(query_weight.shape, BF16),
            pltpu.VMEM((d, 2 * hd), BF16),
            pltpu.VMEM((NX, heads, n, hd), BF16),
            pltpu.VMEM((NZ, kv_rows, 2 * hd), BF16),
            pltpu.VMEM((NZ * n_ctx, 2 * hd), BF16),
            pltpu.VMEM((NX, heads, n, hd), F32),
            pltpu.VMEM((NX, heads, n, hd), F32),
            pltpu.VMEM((NX, heads, n, hd), F32),
            pltpu.VMEM((NX - 1, heads, 2, n // 2, hd), BF16),
            pltpu.VMEM((NX - 1, heads, 2, n // hd // 2, hd), F32),
            pltpu.VMEM((2, heads, 2, n // 2, hd), BF16),
            pltpu.VMEM((2, heads, 2, n // hd // 2, hd), F32),
            pltpu.VMEM((2, 2, n // 2, hd), BF16),
            pltpu.VMEM((2, 2, n // hd // 2, hd), F32),
            pltpu.VMEM((NTP,) + out_weight.shape, BF16),
            pltpu.VMEM((n, heads * hd), BF16),
            pltpu.VMEM((NTP, mine, heads * hd), BF16),
            pltpu.VMEM((mine, d), F32),
            dma((15,)),
        ]
        + pairs,
        compiler_params=pltpu.CompilerParams(
            collective_id=0, has_side_effects=True, vmem_limit_bytes=62 * 1024 * 1024
        ),
    )(*inputs)


def solution(mesh):
    torus = Mesh(mesh.devices.reshape(NZ, NX, NY, NC), ("z", "x", "y", "c"))
    sp, tp = ("z", "x"), ("y", "c")
    placed = (
        P(sp + tp, None),
        P(sp, None),
        P(sp),
        P(sp),
        P(sp, tp),
        P(None, tp),
        P(None, tp),
        P(None, tp),
        P(tp, None),
        P(),
        P(),
    )
    return jax.shard_map(body, mesh=torus, in_specs=placed, out_specs=P(sp + tp, None), check_vma=False)
```

```python
import functools
import math

import jax
import jax.numpy as jnp
import numpy as np
from jax import lax
from jax.experimental import pallas as pl
from jax.experimental.pallas import tpu as pltpu
from jax.sharding import Mesh
from jax.sharding import PartitionSpec as P

MESH_ID = pl.DeviceIdType.MESH
GRID_W = 64
NORM_EPS = 1e-06
ROPE_BASE = 10000.0
NZ, NX, NY, NC = 8, 4, 4, 2
NTP = NY * NC
BF16, F32 = jnp.bfloat16, jnp.float32
VMEM_SPEC = pl.BlockSpec(memory_space=pltpu.VMEM)


def remote(src, dst, send_sem, recv_sem, **to):
    return pltpu.make_async_remote_copy(
        src_ref=src,
        dst_ref=dst,
        send_sem=send_sem,
        recv_sem=recv_sem,
        device_id=to,
        device_id_type=MESH_ID,
    )


class View:
    def __init__(self, ref, index=None):
        self.ref, self.index = ref, index

    def __getitem__(self, index):
        return View(self.ref, index)


def make(*args, **to):
    return remote(*(a.ref.at[a.index] if isinstance(a, View) else a for a in args), **to)


def greet(peers):
    barrier = pltpu.get_barrier_semaphore()
    for peer in peers:
        pl.semaphore_signal(barrier, inc=1, device_id=peer, device_id_type=MESH_ID)
    return functools.partial(pl.semaphore_wait, barrier, len(peers))


def tp_peers(y, c):
    peers = [{"c": 1 - c}]
    for dy in range(1, NY):
        for dc in range(NC):
            peers.append({"y": lax.rem(y + dy, NY), "c": lax.rem(c + dc, NC)})
    return peers


def tp_index(peer, y, c):
    return peer.get("y", y) * NC + peer["c"]


def diagonal(n):
    return lax.broadcasted_iota(jnp.int32, (n, n), 0) == lax.broadcasted_iota(jnp.int32, (n, n), 1)


def rope_tables(row_tokens, freqs):
    c = freqs // 4
    inv = (ROPE_BASE ** (-np.arange(c, dtype=np.float32) / np.float32(c))).astype(np.float32)

    def table(count, lanes_from):
        angles = np.arange(count, dtype=np.float32)[:, None] * inv[None, :]
        cos, sin = np.cos(angles), np.sin(angles)
        out_c = np.zeros((count, freqs), np.float32)
        out_s = np.zeros((count, freqs), np.float32)
        out_c[:, lanes_from : lanes_from + 2 * c] = np.concatenate([cos, cos], 1)
        out_s[:, lanes_from : lanes_from + 2 * c] = np.concatenate([-sin, sin], 1)
        return out_c, out_s

    return table(row_tokens, 0) + table(GRID_W, freqs // 2)


def rms(v):
    return v * lax.rsqrt(jnp.mean(v * v, axis=-1, keepdims=True) + NORM_EPS)


def block_kernel(
    lift,
    *refs,
):
    (
        lat_hbm,
        ctx_hbm,
        cond_hbm,
        ctx_cond_hbm,
        mod_weight_hbm,
        qg_hbm,
        kg_hbm,
        row_c_hbm,
        row_s_hbm,
        col_c_hbm,
        col_s_hbm,
        wq_hbm,
        wk_hbm,
        wv_hbm,
        w_hbm,
        out,
        *refs,
    ) = refs
    (lat, ctx, cond, ctx_cond, mod_weight, qg, kg, row_c, row_s, col_c, col_s, *refs) = refs
    (
    rows,
    normed,
    mod,
    part,
    px,
    pt,
    zbuf,
    xbuf,
    tbuf,
    wq,
    wkv,
    qbuf,
    kvbuf,
    cbuf,
    acc,
    top,
    tot,
    osend,
    lsend,
    orecv,
    lrecv,
    orelay,
    lrelay,
    wfull,
    att,
    exch,
    mixed,
    loc,
    rs,
    rr,
    zs,
    zr,
    xs,
    xr,
    ms,
    mr,
    ks,
    kr,
    qs,
    qr,
    ws,
    wr,
    os_,
    or_,
    ls_,
    lr_,
    ts,
    tr,
    ) = refs
    z, x, y, c = (lax.axis_index(a) for a in ("z", "x", "y", "c"))
    me = y * NC + c
    zp, zm = lax.rem(z + 1, NZ), lax.rem(z + NZ - 1, NZ)
    xp, xm = lax.rem(x + 1, NX), lax.rem(x + NX - 1, NX)
    yp, ym = lax.rem(y + 1, NY), lax.rem(y + NY - 1, NY)
    low, high, far = ym * NC + c, yp * NC + c, lax.rem(y + 2, NY) * NC + c
    mine, d = lat.shape
    heads, n, hd = qbuf.shape[1:]
    n_ctx = ctx.shape[0]
    scale = hd ** (-0.5) * math.log2(math.e)
    raw_lift = lift / hd ** (-0.5)


    z_to = [{"z": lax.rem(z + i, NZ)} for i in range(1, NZ)]
    x_to = [{"x": lax.rem(x + i, NX)} for i in range(1, NX)]
    t_to = tp_peers(y, c)
    greeted = greet(z_to + x_to + t_to)

    fetches = (
        (lat_hbm, lat),
        (mod_weight_hbm, mod_weight),
        (cond_hbm, cond),
        (ctx_cond_hbm, ctx_cond),
        (wk_hbm, wkv.at[:, 0:hd]),
        (wv_hbm, wkv.at[:, hd : 2 * hd]),
        (ctx_hbm, ctx),
        (row_c_hbm, row_c),
        (row_s_hbm, row_s),
        (col_c_hbm, col_c),
        (col_s_hbm, col_s),
        (qg_hbm, qg),
        (kg_hbm, kg),
        (wq_hbm, wq),
        (w_hbm, wfull.at[me]),
    )
    fetch = [pltpu.make_async_copy(src, dst, loc.at[i]) for i, (src, dst) in enumerate(fetches)]
    for cp in fetch:
        cp.start()
    for cp in fetch[0:4]:
        cp.wait()

    def go(src, dst, sems, i, **to):
        make(src, dst, View(sems[0])[0], View(sems[1])[i], **to).start()

    def got(view, sems, i):
        make(view, view, View(sems[0])[0], View(sems[1])[i], c=1 - c).wait_recv()

    def gone(view, sems):
        make(view, view, View(sems[0])[0], View(sems[1])[0], c=1 - c).wait_send()

    r_, z_, x_, m_, k_, q_, w_, o_, l_, t_ = (
        (rs, rr), (zs, zr), (xs, xr), (ms, mr), (ks, kr), (qs, qr), (ws, wr), (os_, or_), (ls_, lr_), (ts, tr),
    )

    rh = mine // 2
    rpiece = (pl.ds(0, rh), pl.ds(rh, rh))

    def r_to(src, row, p, i, **to):
        go(src, View(rows)[row, rpiece[p]], r_, i, **to)

    eye_in = diagonal(cond.shape[1])
    for r, ref in enumerate((cond, ctx_cond)):
        v = ref[...]
        v = v * jax.nn.sigmoid(v)
        column = jnp.sum(jnp.where(eye_in, jnp.broadcast_to(v, eye_in.shape), 0.0), axis=1, keepdims=True)
        part[r : r + 1, :] = jnp.sum(column * mod_weight[...], axis=0, keepdims=True)
    rows[me] = lat[...]
    acc[...] = jnp.zeros_like(acc)
    tot[...] = jnp.zeros_like(tot)
    top[...] = jnp.full_like(top, -1e30)
    greeted()

    for i in (3, 2, 4, 1, 5, 0, 6):
        go(part, View(zbuf)[z], z_, 0, **z_to[i])
    for i in range(2):
        r_to(View(lat)[rpiece[i]], me, i, i, y=yp)
        r_to(View(lat)[rpiece[1 - i]], me, 1 - i, i, y=ym)
    go(lat, View(rows)[me], r_, 3, c=1 - c)
    zbuf[z] = part[...]
    got(View(zbuf)[0 : NZ - 1], z_, 0)
    px[...] = sum((zbuf[i] for i in range(1, NZ)), zbuf[0])
    for to in x_to:
        go(px, View(xbuf)[x], x_, 0, **to)
    xbuf[x] = px[...]
    got(View(rows)[0], r_, 0)
    r_to(View(rows)[low, rpiece[0]], low, 0, 2, y=yp)
    r_to(View(rows)[high, rpiece[1]], high, 1, 2, y=ym)
    got(View(xbuf)[0 : NX - 1], x_, 0)
    pt[...] = sum((xbuf[i] for i in range(1, NX)), xbuf[0])
    for to in t_to:
        go(pt, View(tbuf)[me], m_, 0, **to)
    tbuf[me] = pt[...]
    got(View(rows)[0], r_, 1)
    go(View(rows)[low], View(rows)[low], r_, 3, c=1 - c)
    go(View(rows)[high], View(rows)[high], r_, 3, c=1 - c)
    got(View(rows)[0], r_, 2)
    go(View(rows)[far], View(rows)[far], r_, 3, c=1 - c)
    for cp in fetch[4:]:
        cp.wait()

    wh = w_hbm.shape[0] // 2
    wpiece = (pl.ds(0, wh), pl.ds(wh, wh))

    def w_to(row, p, i, **to):
        piece = View(wfull)[row, wpiece[p]]
        go(piece, piece, w_, i, **to)

    for i in range(2):
        w_to(me, i, i, y=yp)
        w_to(me, 1 - i, i, y=ym)
    go(View(wfull)[me], View(wfull)[me], w_, 3, c=1 - c)
    got(View(tbuf)[0 : NTP - 1], m_, 0)
    w = part.shape[1]
    for i in range(NTP):
        mod[:, i * w : (i + 1) * w] = tbuf[i]
    got(View(rows)[0:4], r_, 3)

    cut = n // 2
    quarter = n // 4
    kpiece = [pl.ds(p * quarter, quarter) for p in range(3)] + [pl.ds(3 * quarter, quarter + n_ctx)]
    plus, minus = (0, 1, 2, 3), (2, 3, 0, 1)

    def k_to(src, slot, p, **to):
        order = plus if slot % 2 else minus
        i = 12 if slot == NZ - 1 else 4 * ((slot - 1) // 2) + order.index(p)
        go(View(kvbuf)[src, kpiece[p]], View(kvbuf)[slot, kpiece[p]], k_, i, **to)

    def k_got(hop, i):
        count = kpiece[plus[i]].size + kpiece[minus[i]].size
        got(View(kvbuf)[0, 0:count], k_, 4 * (hop - 1) + i)

    def q_to(src, slot, h, i, **to):
        go(View(qbuf)[src, h], View(qbuf)[slot, h], q_, i, **to)

    def modulated(v, r):
        v = rms(v.astype(F32))
        return (v * (1.0 + mod[r : r + 1, d : 2 * d]) + mod[r : r + 1, 0:d]).astype(BF16)

    groups = cut // GRID_W
    first = (z * NX + x) * (n // GRID_W)
    lane = lax.broadcasted_iota(jnp.int32, (cut, hd), 1)
    early = lax.rem(lane, hd // 2) < hd // 4

    def table(row_table, col_table, i):
        at = [first + i * groups + g for g in range(groups)]
        return jnp.concatenate([row_table[pl.ds(t, 1), :] + col_table[...] for t in at], axis=0)

    def turned(v, i):
        other = jnp.where(early, pltpu.roll(v, hd - hd // 4, 1), pltpu.roll(v, hd // 4, 1))
        return (v * table(row_c, col_c, i) + other * table(row_s, col_s, i)).astype(BF16)

    per = NTP // 2
    for i in range(2):
        for g in range(per):
            normed[i * per + g] = modulated(rows[i * per + g], 0)
        a = normed[i * per : (i + 1) * per].reshape(cut, d)
        kv = jnp.dot(a, wkv[...], preferred_element_type=F32)
        at = slice(i * cut, (i + 1) * cut)
        kvbuf[0, at, 0:hd] = turned(rms(kv[:, 0:hd]) * kg[...], i)
        kvbuf[0, at, hd : 2 * hd] = kv[:, hd : 2 * hd].astype(BF16)
        if i == 1:
            kv = jnp.dot(modulated(ctx[...], 1), wkv[...], preferred_element_type=F32)
            kvbuf[0, n : n + n_ctx, 0:hd] = (rms(kv[:, 0:hd]) * kg[...]).astype(BF16)
            kvbuf[0, n : n + n_ctx, hd : 2 * hd] = kv[:, hd : 2 * hd].astype(BF16)
        for p in plus[2 * i : 2 * i + 2]:
            k_to(0, 1, p, z=zp)
        if i == 1:
            for p in minus:
                k_to(0, 2, p, z=zm)
    def queries(i, carry):
        a = normed[pl.ds(i * per, per)].reshape(cut, d)
        q = jnp.dot(a, wq[...], preferred_element_type=F32)
        at = pl.ds(pl.multiple_of(i * cut, cut), cut)
        for h in range(heads):
            qbuf[0, h, at, :] = turned(rms(q[:, h * hd : (h + 1) * hd]) * qg[...], i)
        return carry

    lax.fori_loop(0, 2, queries, 0)
    for i in range(2):
        q_to(0, 1, i, i, x=xp)
        q_to(0, 2, 1 - i, i, x=xm)

    def scores(a, h, k):
        return lax.dot_general(qbuf[a, h], k, (((1,), (1,)), ((), ())), preferred_element_type=F32)

    def update(a, h, s, v):
        wide = s.shape[1] // hd
        old = top[a, h]
        new = jnp.maximum(old, jnp.max(s, axis=1, keepdims=True))
        factor = jnp.exp2((old - new) * scale)
        p = jnp.exp2((s - jnp.concatenate([new] * wide, axis=1)) * scale)
        some = sum((p[:, i * hd : (i + 1) * hd] for i in range(1, wide)), p[:, 0:hd])
        top[a, h] = new
        tot[a, h] = tot[a, h] * factor + some
        acc[a, h] = acc[a, h] * factor + jnp.dot(p.astype(BF16), v, preferred_element_type=F32)

    def tile(works, slots, tail=False):
        spans = [b if isinstance(b, tuple) else (b, 0, n) for b in slots]
        m = sum(hi - lo for _, lo, hi in spans)

        def take(lane):
            at = slice(lane, lane + hd)
            return jnp.concatenate([kvbuf[b, lo:hi, at] for b, lo, hi in spans] + ([cbuf[:, at]] if tail else []), axis=0)

        k, v = take(0), take(hd)
        found = [scores(a, h, k) for a, h in works]
        for (a, h), s in zip(works, found):
            if tail:
                s = jnp.concatenate([s[:, 0:m], s[:, m:] + raw_lift], axis=1)
            update(a, h, s, v)

    def both_heads(a):
        return [(a, h) for h in range(heads)]

    eye = diagonal(hd)
    blocks = n // hd

    parts = 2
    pb = blocks // parts

    def join(a, h, t, others, o_to, l_to):
        for b in range(pb):
            at = pl.ds((t * pb + b) * hd, hd)
            here = pl.ds(b * hd, hd)
            total = jnp.sum(tot[a, h, at, :], axis=1, keepdims=True)
            value = acc[a, h, at, :] / total
            lse = top[a, h, at, :] * scale + jnp.log2(total)
            if others:
                lses, values = [lse], [value]
                for o_ref, l_ref in others:
                    row = jnp.broadcast_to(l_ref[b : b + 1, :], (hd, hd))
                    col = jnp.sum(jnp.where(eye, row, 0.0), axis=1, keepdims=True)
                    lses.append(jnp.broadcast_to(col, (hd, hd)))
                    values.append(o_ref[here, :].astype(F32))
                best = functools.reduce(jnp.maximum, lses)
                weights = [jnp.exp2(v - best) for v in lses]
                total = sum(weights[1:], weights[0])
                value = sum((w * v for w, v in zip(weights[1:], values[1:])), weights[0] * values[0]) / total
                lse = best + jnp.log2(total)
            o_to(b, value.astype(BF16))
            if l_to is not None:
                l_to[b : b + 1, :] = jnp.sum(jnp.where(eye, lse, 0.0), axis=0, keepdims=True)

    def finish(a, h, t, others=()):
        def put(b, value):
            osend[a - 1, h, t, b * hd : (b + 1) * hd, :] = value

        join(a, h, t, others, put, lsend.at[a - 1, h, t])

    def o_go(a, h, t, to_o, to_l, i, **to):
        go(View(lsend)[a - 1, h, t], to_l, l_, i, **to)
        go(View(osend)[a - 1, h, t], to_o, o_, i, **to)

    def o_got(o_view, l_view, i):
        got(l_view, l_, i)
        got(o_view, o_, i)

    def pass_on(hop, i):
        src_p, src_m = 2 * hop - 1, 2 * hop
        k_got(hop, i)
        k_to(src_p, src_p + 2, plus[i], z=zp)
        k_to(src_m, src_p + 2 if hop == 3 else src_m + 2, minus[i], z=zm)

    tile(both_heads(0), (0,))
    pass_on(1, 0)
    pass_on(1, 1)
    tile(both_heads(0), ((1, 0, cut), (2, cut, n)))
    pass_on(1, 2)
    pass_on(1, 3)
    got(View(qbuf)[1], q_, 0)
    q_to(1, 3, 0, 2, x=xp)
    q_to(2, 3, 1, 2, x=xm)
    tile(both_heads(0), ((1, cut, n), (2, 0, cut)))
    got(View(qbuf)[1], q_, 1)

    for a in range(1, 4):
        if a < 3:
            pass_on(2, a - 1)
        else:
            pass_on(2, 2)
            pass_on(2, 3)
            got(View(qbuf)[1], q_, 2)
        tile(both_heads(a), (0, 1, 2))
    for a in range(1, 4):
        if a < 3:
            pass_on(3, a - 1)
        if a == 2:
            got(View(wfull)[0], w_, 0)
            w_to(low, 0, 2, y=yp)
            w_to(high, 1, 2, y=ym)
        tile(both_heads(a), (3, 4))
    k_got(3, 2)
    k_got(3, 3)
    tile(both_heads(3), (5, 6))
    got(View(kvbuf)[0], k_, 12)
    for b in range(NZ):
        cbuf[b * n_ctx : (b + 1) * n_ctx, :] = kvbuf[b, n : n + n_ctx, :]

    late = (5, 6, 7)
    tile(both_heads(3), (7,), True)
    for t in range(parts):
        finish(3, 0, t)
        finish(3, 1, t)
        o_go(3, 0, t, View(orelay)[0, t], View(lrelay)[0, t], t, x=xp)
        o_go(3, 1, t, View(orelay)[1, t], View(lrelay)[1, t], t, x=xm)

    tile([(1, 0), (2, 1)], late, True)
    for t in range(parts):
        finish(1, 0, t)
        finish(2, 1, t)
        o_go(1, 0, t, View(orecv)[1, 0, t], View(lrecv)[1, 0, t], parts + t, x=xm)
        o_go(2, 1, t, View(orecv)[0, 1, t], View(lrecv)[0, 1, t], parts + t, x=xp)
    tile([(2, 0), (1, 1)], late, True)
    got(View(wfull)[0], w_, 1)
    go(View(wfull)[low], View(wfull)[low], w_, 4, c=1 - c)
    go(View(wfull)[high], View(wfull)[high], w_, 4, c=1 - c)
    for t in range(parts):
        o_got(View(orelay)[0], View(lrelay)[0], t)
        finish(2, 0, t, [(orelay.at[0, t], lrelay.at[0, t])])
        finish(1, 1, t, [(orelay.at[1, t], lrelay.at[1, t])])
        o_go(2, 0, t, View(orecv)[0, 0, t], View(lrecv)[0, 0, t], parts + t, x=xp)
        o_go(1, 1, t, View(orecv)[1, 1, t], View(lrecv)[1, 1, t], parts + t, x=xm)
    tile(both_heads(0), (3, 4))
    tile(both_heads(0), late, True)
    got(View(wfull)[0], w_, 2)
    go(View(wfull)[far], View(wfull)[far], w_, 5, c=1 - c)

    for t in range(parts):
        o_got(View(orecv)[0], View(lrecv)[0], parts + t)
        for h in range(heads):

            def put(b, value, h=h, t=t):
                att[(t * pb + b) * hd : (t * pb + b + 1) * hd, h * hd : (h + 1) * hd] = value

            join(0, h, t, [(orecv.at[i, h, t], lrecv.at[i, h, t]) for i in range(2)], put, None)

    for i in (3, 4, 1, 2, 5, 6, 0):
        at = pl.multiple_of(tp_index(t_to[i], y, c) * mine, mine)
        go(View(att)[pl.ds(at, mine), :], View(exch)[me], t_, i, **t_to[i])
    exch[me] = att[pl.ds(pl.multiple_of(me * mine, mine), mine), :]

    def add(source, fresh=False):
        product = jnp.dot(exch[source], wfull[source], preferred_element_type=F32)
        mixed[...] = product if fresh else mixed[...] + product

    def came(i):
        got(View(exch)[0], t_, i)
        back = {1: 5, 2: 6, 5: 1, 6: 2}.get(i, i)
        add(tp_index(t_to[back], y, c))

    add(me, True)
    got(View(wfull)[0], w_, 3)
    came(0)
    got(View(wfull)[0:2], w_, 4)
    for i in (1, 2, 5, 6):
        came(i)
    got(View(wfull)[0], w_, 5)
    for i in (3, 4):
        came(i)
    out[...] = (lat[...].astype(F32) + mod[0:1, 2 * d : 3 * d] * rms(mixed[...])).astype(BF16)
    sent = (
        (View(rows)[0 : NTP - 1], r_),
        (View(zbuf)[0 : NZ - 1], z_),
        (View(xbuf)[0 : NX - 1], x_),
        (View(tbuf)[0 : NTP - 1], m_),
        (View(kvbuf)[1:NZ], k_),
        (View(qbuf)[1:NX], q_),
        (View(wfull)[0 : NTP - 1], w_),
        (osend, o_),
        (lsend, l_),
        (View(exch)[0 : NTP - 1], t_),
    )
    for view, sems in sent:
        gone(view, sems)


def body(
    latents,
    context,
    cond,
    ctx_cond,
    mod_weight,
    query_weight,
    key_matrix,
    value_matrix,
    out_weight,
    query_gain,
    key_gain,
):
    mine, d = latents.shape
    n_ctx = context.shape[0]
    hd = query_gain.shape[0]
    heads = query_weight.shape[1] // hd
    n = mine * NTP
    kv_rows = n + n_ctx
    cols = mod_weight.shape[1]
    tokens = n * NZ * NX
    lift = math.log(tokens / (2.0 * n_ctx * NZ * NX))
    tables = [jnp.asarray(t) for t in rope_tables(tokens // GRID_W, hd)]
    dma = pltpu.SemaphoreType.DMA
    kinds = (4, 1, 1, 1, 13, 3, 6, 4, 4, NTP - 1)
    pairs = [dma((c,)) for count in kinds for c in (1, count)]
    inputs = (
        latents,
        context,
        cond[None, :],
        ctx_cond[None, :],
        mod_weight,
        query_gain[None, :],
        key_gain[None, :],
        *tables,
        query_weight,
        key_matrix,
        value_matrix,
        out_weight,
    )
    return pl.pallas_call(
        functools.partial(block_kernel, lift),
        name="block_stage",
        out_shape=pltpu.VMEM((mine, d), BF16),
        in_specs=[pl.BlockSpec(memory_space=pl.ANY)] * len(inputs),
        out_specs=VMEM_SPEC,
        scratch_shapes=[pltpu.VMEM(a.shape, a.dtype) for a in inputs[:11]]
        + [
            pltpu.VMEM((NTP, mine, d), BF16),
            pltpu.VMEM((NTP, mine, d), BF16),
            pltpu.VMEM((2, NTP * cols), F32),
            pltpu.VMEM((2, cols), F32),
            pltpu.VMEM((2, cols), F32),
            pltpu.VMEM((2, cols), F32),
            pltpu.VMEM((NZ, 2, cols), F32),
            pltpu.VMEM((NX, 2, cols), F32),
            pltpu.VMEM((NTP, 2, cols), F32),
            pltpu.VMEM(query_weight.shape, BF16),
            pltpu.VMEM((d, 2 * hd), BF16),
            pltpu.VMEM((NX, heads, n, hd), BF16),
            pltpu.VMEM((NZ, kv_rows, 2 * hd), BF16),
            pltpu.VMEM((NZ * n_ctx, 2 * hd), BF16),
            pltpu.VMEM((NX, heads, n, hd), F32),
            pltpu.VMEM((NX, heads, n, hd), F32),
            pltpu.VMEM((NX, heads, n, hd), F32),
            pltpu.VMEM((NX - 1, heads, 2, n // 2, hd), BF16),
            pltpu.VMEM((NX - 1, heads, 2, n // hd // 2, hd), F32),
            pltpu.VMEM((2, heads, 2, n // 2, hd), BF16),
            pltpu.VMEM((2, heads, 2, n // hd // 2, hd), F32),
            pltpu.VMEM((2, 2, n // 2, hd), BF16),
            pltpu.VMEM((2, 2, n // hd // 2, hd), F32),
            pltpu.VMEM((NTP,) + out_weight.shape, BF16),
            pltpu.VMEM((n, heads * hd), BF16),
            pltpu.VMEM((NTP, mine, heads * hd), BF16),
            pltpu.VMEM((mine, d), F32),
            dma((15,)),
        ]
        + pairs,
        compiler_params=pltpu.CompilerParams(
            collective_id=0, has_side_effects=True, vmem_limit_bytes=62 * 1024 * 1024
        ),
    )(*inputs)


def solution(mesh):
    torus = Mesh(mesh.devices.reshape(NZ, NX, NY, NC), ("z", "x", "y", "c"))
    sp, tp = ("z", "x"), ("y", "c")
    placed = (
        P(sp + tp, None),
        P(sp, None),
        P(sp),
        P(sp),
        P(sp, tp),
        P(None, tp),
        P(None, tp),
        P(None, tp),
        P(tp, None),
        P(),
        P(),
    )
    return jax.shard_map(body, mesh=torus, in_specs=placed, out_specs=P(sp + tp, None), check_vma=False)
```

```python
import functools
import math

import jax
import jax.numpy as jnp
import numpy as np
from jax import lax
from jax.experimental import pallas as pl
from jax.experimental.pallas import tpu as pltpu
from jax.sharding import Mesh
from jax.sharding import PartitionSpec as P

MESH_ID = pl.DeviceIdType.MESH
GRID_W = 64
NORM_EPS = 1e-06
ROPE_BASE = 10000.0
NZ, NX, NY, NC = 8, 4, 4, 2
NTP = NY * NC
BF16, F32 = jnp.bfloat16, jnp.float32
VMEM_SPEC = pl.BlockSpec(memory_space=pltpu.VMEM)


def remote(src, dst, send_sem, recv_sem, **to):
    return pltpu.make_async_remote_copy(
        src_ref=src,
        dst_ref=dst,
        send_sem=send_sem,
        recv_sem=recv_sem,
        device_id=to,
        device_id_type=MESH_ID,
    )


class View:
    def __init__(self, ref, index=None):
        self.ref, self.index = ref, index

    def __getitem__(self, index):
        return View(self.ref, index)


def make(*args, **to):
    return remote(*(a.ref.at[a.index] if isinstance(a, View) else a for a in args), **to)


def greet(peers):
    barrier = pltpu.get_barrier_semaphore()
    for peer in peers:
        pl.semaphore_signal(barrier, inc=1, device_id=peer, device_id_type=MESH_ID)
    return functools.partial(pl.semaphore_wait, barrier, len(peers))


def tp_peers(y, c):
    peers = [{"c": 1 - c}]
    for dy in range(1, NY):
        for dc in range(NC):
            peers.append({"y": lax.rem(y + dy, NY), "c": lax.rem(c + dc, NC)})
    return peers


def tp_index(peer, y, c):
    return peer.get("y", y) * NC + peer["c"]


def diagonal(n):
    return lax.broadcasted_iota(jnp.int32, (n, n), 0) == lax.broadcasted_iota(jnp.int32, (n, n), 1)


def rope_tables(row_tokens, freqs):
    c = freqs // 4
    inv = (ROPE_BASE ** (-np.arange(c, dtype=np.float32) / np.float32(c))).astype(np.float32)

    def table(count, lanes_from):
        angles = np.arange(count, dtype=np.float32)[:, None] * inv[None, :]
        cos, sin = np.cos(angles), np.sin(angles)
        out_c = np.zeros((count, freqs), np.float32)
        out_s = np.zeros((count, freqs), np.float32)
        out_c[:, lanes_from : lanes_from + 2 * c] = np.concatenate([cos, cos], 1)
        out_s[:, lanes_from : lanes_from + 2 * c] = np.concatenate([-sin, sin], 1)
        return out_c, out_s

    return table(row_tokens, 0) + table(GRID_W, freqs // 2)


def rms(v):
    return v * lax.rsqrt(jnp.mean(v * v, axis=-1, keepdims=True) + NORM_EPS)


def block_kernel(
    lift,
    *refs,
):
    (
        lat_hbm,
        ctx_hbm,
        cond_hbm,
        ctx_cond_hbm,
        mod_weight_hbm,
        qg_hbm,
        kg_hbm,
        row_c_hbm,
        row_s_hbm,
        col_c_hbm,
        col_s_hbm,
        wq_hbm,
        wk_hbm,
        wv_hbm,
        w_hbm,
        out,
        *refs,
    ) = refs
    (lat, ctx, cond, ctx_cond, mod_weight, qg, kg, row_c, row_s, col_c, col_s, *refs) = refs
    (
    rows,
    normed,
    mod,
    part,
    px,
    pt,
    zbuf,
    xbuf,
    tbuf,
    wq,
    wkv,
    qbuf,
    kvbuf,
    cbuf,
    acc,
    top,
    tot,
    osend,
    lsend,
    orecv,
    lrecv,
    orelay,
    lrelay,
    wfull,
    att,
    exch,
    mixed,
    loc,
    rs,
    rr,
    zs,
    zr,
    xs,
    xr,
    ms,
    mr,
    ks,
    kr,
    qs,
    qr,
    ws,
    wr,
    os_,
    or_,
    ls_,
    lr_,
    ts,
    tr,
    ) = refs
    z, x, y, c = (lax.axis_index(a) for a in ("z", "x", "y", "c"))
    me = y * NC + c
    zp, zm = lax.rem(z + 1, NZ), lax.rem(z + NZ - 1, NZ)
    xp, xm = lax.rem(x + 1, NX), lax.rem(x + NX - 1, NX)
    yp, ym = lax.rem(y + 1, NY), lax.rem(y + NY - 1, NY)
    low, high, far = ym * NC + c, yp * NC + c, lax.rem(y + 2, NY) * NC + c
    mine, d = lat.shape
    heads, n, hd = qbuf.shape[1:]
    n_ctx = ctx.shape[0]
    scale = hd ** (-0.5) * math.log2(math.e)
    raw_lift = lift / hd ** (-0.5)


    z_to = [{"z": lax.rem(z + i, NZ)} for i in range(1, NZ)]
    x_to = [{"x": lax.rem(x + i, NX)} for i in range(1, NX)]
    t_to = tp_peers(y, c)
    greeted = greet(z_to + x_to + t_to)

    fetches = (
        (lat_hbm, lat),
        (mod_weight_hbm, mod_weight),
        (cond_hbm, cond),
        (ctx_cond_hbm, ctx_cond),
        (wk_hbm, wkv.at[:, 0:hd]),
        (wv_hbm, wkv.at[:, hd : 2 * hd]),
        (ctx_hbm, ctx),
        (row_c_hbm, row_c),
        (row_s_hbm, row_s),
        (col_c_hbm, col_c),
        (col_s_hbm, col_s),
        (qg_hbm, qg),
        (kg_hbm, kg),
        (wq_hbm, wq),
        (w_hbm, wfull.at[me]),
    )
    fetch = [pltpu.make_async_copy(src, dst, loc.at[i]) for i, (src, dst) in enumerate(fetches)]
    for cp in fetch:
        cp.start()
    for cp in fetch[0:4]:
        cp.wait()

    def go(src, dst, sems, i, **to):
        make(src, dst, View(sems[0])[0], View(sems[1])[i], **to).start()

    def got(view, sems, i):
        make(view, view, View(sems[0])[0], View(sems[1])[i], c=1 - c).wait_recv()

    def gone(view, sems):
        make(view, view, View(sems[0])[0], View(sems[1])[0], c=1 - c).wait_send()

    r_, z_, x_, m_, k_, q_, w_, o_, l_, t_ = (
        (rs, rr), (zs, zr), (xs, xr), (ms, mr), (ks, kr), (qs, qr), (ws, wr), (os_, or_), (ls_, lr_), (ts, tr),
    )

    rh = mine // 2
    rpiece = (pl.ds(0, rh), pl.ds(rh, rh))

    def r_to(src, row, p, i, **to):
        go(src, View(rows)[row, rpiece[p]], r_, i, **to)

    eye_in = diagonal(cond.shape[1])
    for r, ref in enumerate((cond, ctx_cond)):
        v = ref[...]
        v = v * jax.nn.sigmoid(v)
        column = jnp.sum(jnp.where(eye_in, jnp.broadcast_to(v, eye_in.shape), 0.0), axis=1, keepdims=True)
        part[r : r + 1, :] = jnp.sum(column * mod_weight[...], axis=0, keepdims=True)
    rows[me] = lat[...]
    acc[...] = jnp.zeros_like(acc)
    tot[...] = jnp.zeros_like(tot)
    top[...] = jnp.full_like(top, -1e30)
    greeted()

    for i in (3, 2, 4, 1, 5, 0, 6):
        go(part, View(zbuf)[z], z_, 0, **z_to[i])
    for i in range(2):
        r_to(View(lat)[rpiece[i]], me, i, i, y=yp)
        r_to(View(lat)[rpiece[1 - i]], me, 1 - i, i, y=ym)
    go(lat, View(rows)[me], r_, 3, c=1 - c)
    zbuf[z] = part[...]
    got(View(zbuf)[0 : NZ - 1], z_, 0)
    px[...] = sum((zbuf[i] for i in range(1, NZ)), zbuf[0])
    for to in x_to:
        go(px, View(xbuf)[x], x_, 0, **to)
    xbuf[x] = px[...]
    got(View(rows)[0], r_, 0)
    r_to(View(rows)[low, rpiece[0]], low, 0, 2, y=yp)
    r_to(View(rows)[high, rpiece[1]], high, 1, 2, y=ym)
    got(View(xbuf)[0 : NX - 1], x_, 0)
    pt[...] = sum((xbuf[i] for i in range(1, NX)), xbuf[0])
    for to in t_to:
        go(pt, View(tbuf)[me], m_, 0, **to)
    tbuf[me] = pt[...]
    got(View(rows)[0], r_, 1)
    go(View(rows)[low], View(rows)[low], r_, 3, c=1 - c)
    go(View(rows)[high], View(rows)[high], r_, 3, c=1 - c)
    got(View(rows)[0], r_, 2)
    go(View(rows)[far], View(rows)[far], r_, 3, c=1 - c)
    for cp in fetch[4:]:
        cp.wait()

    wh = w_hbm.shape[0] // 2
    wpiece = (pl.ds(0, wh), pl.ds(wh, wh))

    def w_to(row, p, i, **to):
        piece = View(wfull)[row, wpiece[p]]
        go(piece, piece, w_, i, **to)

    for i in range(2):
        w_to(me, i, i, y=yp)
        w_to(me, 1 - i, i, y=ym)
    go(View(wfull)[me], View(wfull)[me], w_, 3, c=1 - c)
    got(View(tbuf)[0 : NTP - 1], m_, 0)
    w = part.shape[1]
    for i in range(NTP):
        mod[:, i * w : (i + 1) * w] = tbuf[i]
    got(View(rows)[0:4], r_, 3)

    cut = n // 2
    quarter = n // 4
    kpiece = [pl.ds(p * quarter, quarter) for p in range(3)] + [pl.ds(3 * quarter, quarter + n_ctx)]
    plus, minus = (0, 1, 2, 3), (2, 3, 0, 1)

    def k_to(src, slot, p, **to):
        order = plus if slot % 2 else minus
        i = 12 if slot == NZ - 1 else 4 * ((slot - 1) // 2) + order.index(p)
        go(View(kvbuf)[src, kpiece[p]], View(kvbuf)[slot, kpiece[p]], k_, i, **to)

    def k_got(hop, i):
        count = kpiece[plus[i]].size + kpiece[minus[i]].size
        got(View(kvbuf)[0, 0:count], k_, 4 * (hop - 1) + i)

    def q_to(src, slot, h, i, **to):
        go(View(qbuf)[src, h], View(qbuf)[slot, h], q_, i, **to)

    def modulated(v, r):
        v = rms(v.astype(F32))
        return (v * (1.0 + mod[r : r + 1, d : 2 * d]) + mod[r : r + 1, 0:d]).astype(BF16)

    first = (z * NX + x) * (n // GRID_W)

    def table(row_table, col_table, begin, count):
        at = [first + begin + g for g in range(count)]
        return jnp.concatenate([row_table[pl.ds(t, 1), :] + col_table[...] for t in at], axis=0)

    def turned(v, begin):
        count = v.shape[0] // GRID_W
        lane = lax.broadcasted_iota(jnp.int32, v.shape, 1)
        early = lax.rem(lane, hd // 2) < hd // 4
        other = jnp.where(early, pltpu.roll(v, hd - hd // 4, 1), pltpu.roll(v, hd // 4, 1))
        cos, sin = table(row_c, col_c, begin, count), table(row_s, col_s, begin, count)
        return (v * cos + other * sin).astype(BF16)

    per = NTP // 4
    for i in (0, 2, 1, 3):
        for g in range(per):
            normed[i * per + g] = modulated(rows[i * per + g], 0)
        a = normed[i * per : (i + 1) * per].reshape(quarter, d)
        kv = jnp.dot(a, wkv[...], preferred_element_type=F32)
        at = slice(i * quarter, (i + 1) * quarter)
        kvbuf[0, at, 0:hd] = turned(rms(kv[:, 0:hd]) * kg[...], i * (quarter // GRID_W))
        kvbuf[0, at, hd : 2 * hd] = kv[:, hd : 2 * hd].astype(BF16)
        if i == 3:
            kv = jnp.dot(modulated(ctx[...], 1), wkv[...], preferred_element_type=F32)
            kvbuf[0, n : n + n_ctx, 0:hd] = (rms(kv[:, 0:hd]) * kg[...]).astype(BF16)
            kvbuf[0, n : n + n_ctx, hd : 2 * hd] = kv[:, hd : 2 * hd].astype(BF16)
        for p in {0: (0,), 1: (1, 2), 2: (), 3: (3,)}[i]:
            k_to(0, 1, p, z=zp)
        for p in {0: (), 1: (), 2: (2,), 3: (3, 0, 1)}[i]:
            k_to(0, 2, p, z=zm)

    def queries(i, carry):
        a = normed[pl.ds(i * 2 * per, 2 * per)].reshape(cut, d)
        q = jnp.dot(a, wq[...], preferred_element_type=F32)
        at = pl.ds(pl.multiple_of(i * cut, cut), cut)
        for h in range(heads):
            qbuf[0, h, at, :] = turned(rms(q[:, h * hd : (h + 1) * hd]) * qg[...], i * (cut // GRID_W))
        return carry

    lax.fori_loop(0, 2, queries, 0)
    for i in range(2):
        q_to(0, 1, i, i, x=xp)
        q_to(0, 2, 1 - i, i, x=xm)

    def scores(a, h, k):
        return lax.dot_general(qbuf[a, h], k, (((1,), (1,)), ((), ())), preferred_element_type=F32)

    def update(a, h, s, v):
        wide = s.shape[1] // hd
        old = top[a, h]
        new = jnp.maximum(old, jnp.max(s, axis=1, keepdims=True))
        factor = jnp.exp2((old - new) * scale)
        p = jnp.exp2((s - jnp.concatenate([new] * wide, axis=1)) * scale)
        some = sum((p[:, i * hd : (i + 1) * hd] for i in range(1, wide)), p[:, 0:hd])
        top[a, h] = new
        tot[a, h] = tot[a, h] * factor + some
        acc[a, h] = acc[a, h] * factor + jnp.dot(p.astype(BF16), v, preferred_element_type=F32)

    def tile(works, slots, tail=False):
        spans = [b if isinstance(b, tuple) else (b, 0, n) for b in slots]
        m = sum(hi - lo for _, lo, hi in spans)

        def take(lane):
            at = slice(lane, lane + hd)
            return jnp.concatenate([kvbuf[b, lo:hi, at] for b, lo, hi in spans] + ([cbuf[:, at]] if tail else []), axis=0)

        k, v = take(0), take(hd)
        found = [scores(a, h, k) for a, h in works]
        for (a, h), s in zip(works, found):
            if tail:
                s = jnp.concatenate([s[:, 0:m], s[:, m:] + raw_lift], axis=1)
            update(a, h, s, v)

    def both_heads(a):
        return [(a, h) for h in range(heads)]

    eye = diagonal(hd)
    blocks = n // hd

    parts = 2
    pb = blocks // parts

    def join(a, h, t, others, o_to, l_to):
        for b in range(pb):
            at = pl.ds((t * pb + b) * hd, hd)
            here = pl.ds(b * hd, hd)
            total = jnp.sum(tot[a, h, at, :], axis=1, keepdims=True)
            value = acc[a, h, at, :] / total
            lse = top[a, h, at, :] * scale + jnp.log2(total)
            if others:
                lses, values = [lse], [value]
                for o_ref, l_ref in others:
                    row = jnp.broadcast_to(l_ref[b : b + 1, :], (hd, hd))
                    col = jnp.sum(jnp.where(eye, row, 0.0), axis=1, keepdims=True)
                    lses.append(jnp.broadcast_to(col, (hd, hd)))
                    values.append(o_ref[here, :].astype(F32))
                best = functools.reduce(jnp.maximum, lses)
                weights = [jnp.exp2(v - best) for v in lses]
                total = sum(weights[1:], weights[0])
                value = sum((w * v for w, v in zip(weights[1:], values[1:])), weights[0] * values[0]) / total
                lse = best + jnp.log2(total)
            o_to(b, value.astype(BF16))
            if l_to is not None:
                l_to[b : b + 1, :] = jnp.sum(jnp.where(eye, lse, 0.0), axis=0, keepdims=True)

    def finish(a, h, t, others=()):
        def put(b, value):
            osend[a - 1, h, t, b * hd : (b + 1) * hd, :] = value

        join(a, h, t, others, put, lsend.at[a - 1, h, t])

    def o_go(a, h, t, to_o, to_l, i, **to):
        go(View(lsend)[a - 1, h, t], to_l, l_, i, **to)
        go(View(osend)[a - 1, h, t], to_o, o_, i, **to)

    def o_got(o_view, l_view, i):
        got(l_view, l_, i)
        got(o_view, o_, i)

    def pass_on(hop, i):
        src_p, src_m = 2 * hop - 1, 2 * hop
        k_got(hop, i)
        k_to(src_p, src_p + 2, plus[i], z=zp)
        k_to(src_m, src_p + 2 if hop == 3 else src_m + 2, minus[i], z=zm)

    tile(both_heads(0), (0,))
    pass_on(1, 0)
    pass_on(1, 1)
    tile(both_heads(0), ((1, 0, cut), (2, cut, n)))
    pass_on(1, 2)
    pass_on(1, 3)
    got(View(qbuf)[1], q_, 0)
    q_to(1, 3, 0, 2, x=xp)
    q_to(2, 3, 1, 2, x=xm)
    tile(both_heads(0), ((1, cut, n), (2, 0, cut)))
    got(View(qbuf)[1], q_, 1)

    for a in range(1, 4):
        if a < 3:
            pass_on(2, a - 1)
        else:
            pass_on(2, 2)
            pass_on(2, 3)
            got(View(qbuf)[1], q_, 2)
        tile(both_heads(a), (0, 1, 2))
    for a in range(1, 4):
        if a < 3:
            pass_on(3, a - 1)
        if a == 2:
            got(View(wfull)[0], w_, 0)
            w_to(low, 0, 2, y=yp)
            w_to(high, 1, 2, y=ym)
        tile(both_heads(a), (3, 4))
    k_got(3, 2)
    k_got(3, 3)
    tile(both_heads(3), (5, 6))
    got(View(kvbuf)[0], k_, 12)
    for b in range(NZ):
        cbuf[b * n_ctx : (b + 1) * n_ctx, :] = kvbuf[b, n : n + n_ctx, :]

    late = (5, 6, 7)
    tile(both_heads(3), (7,), True)
    for t in range(parts):
        finish(3, 0, t)
        finish(3, 1, t)
        o_go(3, 0, t, View(orelay)[0, t], View(lrelay)[0, t], t, x=xp)
        o_go(3, 1, t, View(orelay)[1, t], View(lrelay)[1, t], t, x=xm)

    tile([(1, 0), (2, 1)], late, True)
    for t in range(parts):
        finish(1, 0, t)
        finish(2, 1, t)
        o_go(1, 0, t, View(orecv)[1, 0, t], View(lrecv)[1, 0, t], parts + t, x=xm)
        o_go(2, 1, t, View(orecv)[0, 1, t], View(lrecv)[0, 1, t], parts + t, x=xp)
    tile([(2, 0), (1, 1)], late, True)
    got(View(wfull)[0], w_, 1)
    go(View(wfull)[low], View(wfull)[low], w_, 4, c=1 - c)
    go(View(wfull)[high], View(wfull)[high], w_, 4, c=1 - c)
    for t in range(parts):
        o_got(View(orelay)[0], View(lrelay)[0], t)
        finish(2, 0, t, [(orelay.at[0, t], lrelay.at[0, t])])
        finish(1, 1, t, [(orelay.at[1, t], lrelay.at[1, t])])
        o_go(2, 0, t, View(orecv)[0, 0, t], View(lrecv)[0, 0, t], parts + t, x=xp)
        o_go(1, 1, t, View(orecv)[1, 1, t], View(lrecv)[1, 1, t], parts + t, x=xm)
    tile(both_heads(0), (3, 4))
    tile(both_heads(0), late, True)
    got(View(wfull)[0], w_, 2)
    go(View(wfull)[far], View(wfull)[far], w_, 5, c=1 - c)

    for t in range(parts):
        o_got(View(orecv)[0], View(lrecv)[0], parts + t)
        for h in range(heads):

            def put(b, value, h=h, t=t):
                att[(t * pb + b) * hd : (t * pb + b + 1) * hd, h * hd : (h + 1) * hd] = value

            join(0, h, t, [(orecv.at[i, h, t], lrecv.at[i, h, t]) for i in range(2)], put, None)

    for i in (3, 4, 1, 2, 5, 6, 0):
        at = pl.multiple_of(tp_index(t_to[i], y, c) * mine, mine)
        go(View(att)[pl.ds(at, mine), :], View(exch)[me], t_, i, **t_to[i])
    exch[me] = att[pl.ds(pl.multiple_of(me * mine, mine), mine), :]

    def add(source, fresh=False):
        product = jnp.dot(exch[source], wfull[source], preferred_element_type=F32)
        mixed[...] = product if fresh else mixed[...] + product

    def came(i):
        got(View(exch)[0], t_, i)
        back = {1: 5, 2: 6, 5: 1, 6: 2}.get(i, i)
        add(tp_index(t_to[back], y, c))

    add(me, True)
    got(View(wfull)[0], w_, 3)
    came(0)
    got(View(wfull)[0:2], w_, 4)
    for i in (1, 2, 5, 6):
        came(i)
    got(View(wfull)[0], w_, 5)
    for i in (3, 4):
        came(i)
    out[...] = (lat[...].astype(F32) + mod[0:1, 2 * d : 3 * d] * rms(mixed[...])).astype(BF16)
    sent = (
        (View(rows)[0 : NTP - 1], r_),
        (View(zbuf)[0 : NZ - 1], z_),
        (View(xbuf)[0 : NX - 1], x_),
        (View(tbuf)[0 : NTP - 1], m_),
        (View(kvbuf)[1:NZ], k_),
        (View(qbuf)[1:NX], q_),
        (View(wfull)[0 : NTP - 1], w_),
        (osend, o_),
        (lsend, l_),
        (View(exch)[0 : NTP - 1], t_),
    )
    for view, sems in sent:
        gone(view, sems)


def body(
    latents,
    context,
    cond,
    ctx_cond,
    mod_weight,
    query_weight,
    key_matrix,
    value_matrix,
    out_weight,
    query_gain,
    key_gain,
):
    mine, d = latents.shape
    n_ctx = context.shape[0]
    hd = query_gain.shape[0]
    heads = query_weight.shape[1] // hd
    n = mine * NTP
    kv_rows = n + n_ctx
    cols = mod_weight.shape[1]
    tokens = n * NZ * NX
    lift = math.log(tokens / (2.0 * n_ctx * NZ * NX))
    tables = [jnp.asarray(t) for t in rope_tables(tokens // GRID_W, hd)]
    dma = pltpu.SemaphoreType.DMA
    kinds = (4, 1, 1, 1, 13, 3, 6, 4, 4, NTP - 1)
    pairs = [dma((c,)) for count in kinds for c in (1, count)]
    inputs = (
        latents,
        context,
        cond[None, :],
        ctx_cond[None, :],
        mod_weight,
        query_gain[None, :],
        key_gain[None, :],
        *tables,
        query_weight,
        key_matrix,
        value_matrix,
        out_weight,
    )
    return pl.pallas_call(
        functools.partial(block_kernel, lift),
        name="block_stage",
        out_shape=pltpu.VMEM((mine, d), BF16),
        in_specs=[pl.BlockSpec(memory_space=pl.ANY)] * len(inputs),
        out_specs=VMEM_SPEC,
        scratch_shapes=[pltpu.VMEM(a.shape, a.dtype) for a in inputs[:11]]
        + [
            pltpu.VMEM((NTP, mine, d), BF16),
            pltpu.VMEM((NTP, mine, d), BF16),
            pltpu.VMEM((2, NTP * cols), F32),
            pltpu.VMEM((2, cols), F32),
            pltpu.VMEM((2, cols), F32),
            pltpu.VMEM((2, cols), F32),
            pltpu.VMEM((NZ, 2, cols), F32),
            pltpu.VMEM((NX, 2, cols), F32),
            pltpu.VMEM((NTP, 2, cols), F32),
            pltpu.VMEM(query_weight.shape, BF16),
            pltpu.VMEM((d, 2 * hd), BF16),
            pltpu.VMEM((NX, heads, n, hd), BF16),
            pltpu.VMEM((NZ, kv_rows, 2 * hd), BF16),
            pltpu.VMEM((NZ * n_ctx, 2 * hd), BF16),
            pltpu.VMEM((NX, heads, n, hd), F32),
            pltpu.VMEM((NX, heads, n, hd), F32),
            pltpu.VMEM((NX, heads, n, hd), F32),
            pltpu.VMEM((NX - 1, heads, 2, n // 2, hd), BF16),
            pltpu.VMEM((NX - 1, heads, 2, n // hd // 2, hd), F32),
            pltpu.VMEM((2, heads, 2, n // 2, hd), BF16),
            pltpu.VMEM((2, heads, 2, n // hd // 2, hd), F32),
            pltpu.VMEM((2, 2, n // 2, hd), BF16),
            pltpu.VMEM((2, 2, n // hd // 2, hd), F32),
            pltpu.VMEM((NTP,) + out_weight.shape, BF16),
            pltpu.VMEM((n, heads * hd), BF16),
            pltpu.VMEM((NTP, mine, heads * hd), BF16),
            pltpu.VMEM((mine, d), F32),
            dma((15,)),
        ]
        + pairs,
        compiler_params=pltpu.CompilerParams(
            collective_id=0, has_side_effects=True, vmem_limit_bytes=62 * 1024 * 1024
        ),
    )(*inputs)


def solution(mesh):
    torus = Mesh(mesh.devices.reshape(NZ, NX, NY, NC), ("z", "x", "y", "c"))
    sp, tp = ("z", "x"), ("y", "c")
    placed = (
        P(sp + tp, None),
        P(sp, None),
        P(sp),
        P(sp),
        P(sp, tp),
        P(None, tp),
        P(None, tp),
        P(None, tp),
        P(tp, None),
        P(),
        P(),
    )
    return jax.shard_map(body, mesh=torus, in_specs=placed, out_specs=P(sp + tp, None), check_vma=False)
```
